32 devices in a mesh: ep: 8 (over z, core), tp: 4 (over y, x).
Axes of the slice: x: 2, y: 2, z: 4, core: 2. Of those that a mesh axis runs over, the one named last changes fastest.
Arguments:
- receptance: bfloat16 [2048, 2048], P('ep', 'tp'), may hold values from -6 to 6
- key_tensor: bfloat16 [2048, 2048], P('ep', 'tp'), may hold values from -6 to 6
- value_tensor: bfloat16 [2048, 2048], P('ep', 'tp'), may hold values from -6 to 6
- decay_data_input: bfloat16 [2048, 2048], P('ep', 'tp'), may hold values from -4 to 4
- correction_rate_input: bfloat16 [2048, 2048], P('ep', 'tp'), may hold values from -16 to 6
- mixer_output_gate: bfloat16 [2048, 2048], P('ep', 'tp'), may hold values from -6 to 6
- decay_channel_offset: float32 [2048], P('tp'), may hold values from -16 to -3
- head_norm_gain: float32 [2048], P('tp'), may hold values from 0.1 to 1.9
- self_key_weight: float32 [2048], P('tp'), may hold values from -2 to 2
- mixer_output_weight: bfloat16 [2048, 2048], P('tp'), may hold values from -0.125 to 0.125
- second_batch_rows: bfloat16 [1024, 2048], P('ep'), may hold values from -6 to 6
- routed_expert_index: int32 [1024, 4], P('ep'), may hold values from 0 to 7, all different within a row; in each aligned block of 128 rows (0 to 127, 128 to 255, ...) at most 96 rows name the same one
- routing_output_weight: float32 [1024, 4], P('ep'), may hold values from 0.1 to 1
- expert_norm_gain: float32 [2048], replicated, may hold values from 0.1 to 1.9
- expert_gate_weight: bfloat16 [8, 1024, 2048], P('ep', 'tp'), may hold values from -0.125 to 0.125
- expert_up_weight: bfloat16 [8, 1024, 2048], P('ep', 'tp'), may hold values from -0.125 to 0.125
- expert_down_weight: bfloat16 [8, 1024, 2048], P('ep', None, 'tp'), may hold values from -0.1875 to 0.1875
- common_expert_gate: bfloat16 [1024, 2048], P('tp'), may hold values from -0.125 to 0.125
- common_expert_up: bfloat16 [1024, 2048], P('tp'), may hold values from -0.125 to 0.125
- common_expert_down: bfloat16 [1024, 2048], P(None, 'tp'), may hold values from -0.1875 to 0.1875
Outputs:
- token_mixer_output: bfloat16 [2048, 2048], P(('ep', 'tp'))
- expert_out: bfloat16 [1024, 2048], P('ep', 'tp')
The draws below stay inside these ranges and needn't reach their ends.
Inputs may be any that keep to these rules, and one draw needn't show every extreme that they name: `routed_expert_index`: each row names 4 different experts. Within the rows of one index of ep no expert is named by more than 96 rows, and that bound is met in some index's rows.
All inputs are finite; a program needn't handle non-finite values.
Results may differ from the reference program's by a relative error of at most 0.017.
Values may be sent and summed in bfloat16 or wider, within the bound.
A program may use at most 128 MiB of HBM per device.

```python
import math
import jax
import jax.numpy as jnp
import numpy as np
from jax import lax

MODEL_WIDTH = 2048
HEADS = 32
HEAD_CHANNELS = 64
FF = 1024
TOP = 4
ROWS_EXP = 128
SEQ_MIX = 2048
TOKENS_EXP = 1024
EXPERTS = 8
CAP = 96
N_EP = 8
N_TP = 4


def slow_marks(key):
    picks = jax.random.randint(jax.random.fold_in(key, 7), (HEADS,), 0, 10)
    return picks < 5


def draw_decay_channel_offset(key, part):
    slow_heads = slow_marks(key)
    spread = jax.random.uniform(jax.random.fold_in(key, 11), (HEADS, HEAD_CHANNELS), jnp.float32)
    slow_base = jnp.log(0.4 / SEQ_MIX) + 0.5 - spread
    fast_base = -4.0 + spread
    return jnp.where(slow_heads[:, None], slow_base, fast_base).reshape(MODEL_WIDTH).astype(jnp.float32)


def draw_correction_rate_input(key, part):
    slow_heads = slow_marks(key)
    offset = jnp.where(slow_heads, jnp.log(0.3 * HEAD_CHANNELS / SEQ_MIX), 0.0)
    jitter = jnp.clip(jax.random.normal(jax.random.fold_in(key, 13), (SEQ_MIX, HEADS, HEAD_CHANNELS), jnp.float32), -6.0, 6.0)
    return (jitter + offset[None, :, None]).reshape(SEQ_MIX, MODEL_WIDTH).astype(jnp.bfloat16)


def draw_decay_data_input(key, part):
    blocks = SEQ_MIX // 64
    shifts = jax.random.uniform(jax.random.fold_in(key, 17), (blocks, 1, MODEL_WIDTH), jnp.float32, -1.0, 1.0)
    jitter = 0.6 * jnp.clip(jax.random.normal(jax.random.fold_in(key, 19), (blocks, 64, MODEL_WIDTH), jnp.float32), -5.0, 5.0)
    return (jitter + shifts).reshape(SEQ_MIX, MODEL_WIDTH).astype(jnp.bfloat16)


def level_of(own_key, shape, shards, least, top_value):
    loudness, own = 1.0, jax.random.fold_in(own_key, 6)
    for axis_at, blocks in shards:
        draws = jnp.exp(jax.random.uniform(jax.random.fold_in(own, axis_at), (blocks,), jnp.float32, least / len(shards), top_value / len(shards)))
        loudness = loudness * jnp.repeat(draws, shape[axis_at] // blocks).reshape([-1 if axis == axis_at else 1 for axis in range(len(shape))])
    return loudness


def deal_out(own_key, own, number, rows, count, top, reach, slope):
    order = jax.random.permutation(own_key, count)
    crowded, ordinary = portions_of(count, rows * top, reach, slope, True), portions_of(count, rows * top, reach, slope, False)
    places = jnp.arange(count)

    def named(lengths, rotation):
        used = int((lengths > 0).sum())
        fixed = max(1, used // 4)
        moved = fixed + (places - fixed + rotation * (used - fixed)) % max(1, count - fixed)
        return jnp.zeros((count,), jnp.int32).at[order[jnp.where(places < fixed, places, moved)]].set(jnp.asarray(lengths, jnp.int32))

    lengths = jnp.where(number % 4 == 0, named(crowded, number // 4), named(ordinary, number - number // 4 - 1))
    mixed = jax.random.permutation(jax.random.fold_in(own, 3), count)
    source_of, taker = mixed[0:count // 2 * 2:2], mixed[1:count // 2 * 2:2]
    slack = jnp.minimum(lengths[source_of] - 1, reach - lengths[taker]) // 2
    slack = jnp.where((source_of == order[0]) | (taker == order[0]) | (lengths[taker] == 0), 0, jnp.maximum(slack, 0))
    moved = jax.random.randint(jax.random.fold_in(own, 4), (count // 2,), 0, 1 << 20) % (slack + 1)
    lengths = lengths.at[source_of].add(-moved).at[taker].add(moved)
    labels = jnp.searchsorted(jnp.cumsum(lengths), jnp.arange(rows * top), side="right").astype(jnp.int32)
    grid = labels.reshape(top, rows).T
    grid = grid[jax.random.permutation(jax.random.fold_in(own, 1), rows)]
    rotation = jax.random.randint(jax.random.fold_in(own, 2), (rows, 1), 0, top)
    return jnp.take_along_axis(grid, (jnp.arange(top)[None, :] + rotation) % top, axis=1)


def portions_of(amount, total, bound, skew, full):
    loads = [(1 << 20) // math.isqrt(grade ** skew) + 1 for grade in range(1, amount + 1)]
    largest = bound if full else min(bound, max(-(-total // amount), total * loads[0] // sum(loads)))
    least = 1 if total - largest >= amount - 1 else 0
    given, rest = [largest] + [least] * (amount - 1), total - largest - least * (amount - 1)
    while rest > 0:
        candidates = [i for i in range(1, amount) if given[i] < largest] or [i for i in range(1, amount) if given[i] < bound]
        whole, budget = sum([loads[i] for i in candidates]), rest
        for i in candidates:
            extra = min(bound - given[i], max(1, budget * loads[i] // whole), rest)
            given[i] = given[i] + extra
            rest = rest - extra
    return np.array(given)


def noise(own_key, extent, deviation, bound, cuts=(), kind=jnp.bfloat16):
    gain = level_of(own_key, extent, cuts, -0.22, 0.18) if cuts else 1.0
    values = jax.random.normal(own_key, extent, jnp.float32) * deviation * gain
    return jnp.minimum(jnp.maximum(values, -bound), bound).astype(kind)


def setup_inputs(seed: int = 0) -> dict:
    keys = jax.random.split(jax.random.key(seed), 21)
    receptance = noise(keys[0], (SEQ_MIX, MODEL_WIDTH), 1.0, 6.0, ((0, 8), (1, 4)))
    key_tensor = noise(keys[1], (SEQ_MIX, MODEL_WIDTH), 1.0, 6.0, ((0, 8), (1, 4)))
    value_tensor = noise(keys[2], (SEQ_MIX, MODEL_WIDTH), 1.0, 6.0, ((0, 8), (1, 4)))
    decay_data_input = draw_decay_data_input(jax.random.fold_in(keys[20], 71), 0)
    correction_rate_input = draw_correction_rate_input(jax.random.fold_in(keys[20], 71), 0)
    mixer_output_gate = noise(keys[5], (SEQ_MIX, MODEL_WIDTH), 1.0, 6.0, ((0, 8), (1, 4)))
    decay_channel_offset = draw_decay_channel_offset(jax.random.fold_in(keys[20], 71), 0)
    head_norm_gain = jnp.clip(1.0 + 0.18 * jax.random.normal(keys[7], (MODEL_WIDTH,), jnp.float32), 0.1, 1.9)
    self_key_weight = noise(keys[8], (MODEL_WIDTH,), 0.15, 2.0, ((0, 4),), jnp.float32)
    mixer_output_weight = noise(keys[9], (MODEL_WIDTH, MODEL_WIDTH), MODEL_WIDTH ** -0.5, 0.125, ((0, 4),))
    second_batch_rows = noise(keys[10], (TOKENS_EXP, MODEL_WIDTH), 1.0, 6.0, ((0, 8),))
    routed_expert_index_keys = jax.random.split(jax.random.fold_in(keys[11], 1), TOKENS_EXP // ROWS_EXP)
    routed_expert_index_turns = jax.random.permutation(jax.random.fold_in(keys[11], 3), TOKENS_EXP // ROWS_EXP)
    routed_expert_index = jax.vmap(lambda own, number: deal_out(jax.random.fold_in(keys[11], 2), own, number, ROWS_EXP, EXPERTS, TOP, CAP, 1))(routed_expert_index_keys, routed_expert_index_turns).reshape((TOKENS_EXP, TOP))
    routing_output_weight = jnp.clip(0.1 + 0.9 * jax.random.uniform(keys[12], (TOKENS_EXP, TOP), jnp.float32) ** level_of(keys[12], (TOKENS_EXP, TOP), ((0, 8),), -0.2, 0.2), 0.1, 1.0)
    expert_norm_gain = jnp.clip(1.0 + 0.18 * jax.random.normal(keys[13], (MODEL_WIDTH,), jnp.float32), 0.1, 1.9)
    expert_gate_weight = noise(keys[14], (EXPERTS, FF, MODEL_WIDTH), MODEL_WIDTH ** -0.5, 0.125, ((0, 8), (1, 4)))
    expert_up_weight = noise(keys[15], (EXPERTS, FF, MODEL_WIDTH), MODEL_WIDTH ** -0.5, 0.125, ((0, 8), (1, 4)))
    expert_down_weight = noise(keys[16], (EXPERTS, FF, MODEL_WIDTH), FF ** -0.5, 0.1875, ((0, 8), (2, 4)))
    common_expert_gate = noise(keys[17], (FF, MODEL_WIDTH), MODEL_WIDTH ** -0.5, 0.125, ((0, 4),))
    common_expert_up = noise(keys[18], (FF, MODEL_WIDTH), MODEL_WIDTH ** -0.5, 0.125, ((0, 4),))
    common_expert_down = noise(keys[19], (FF, MODEL_WIDTH), FF ** -0.5, 0.1875, ((1, 4),))
    return dict(receptance=receptance, key_tensor=key_tensor, value_tensor=value_tensor, decay_data_input=decay_data_input, correction_rate_input=correction_rate_input, mixer_output_gate=mixer_output_gate, decay_channel_offset=decay_channel_offset, head_norm_gain=head_norm_gain, self_key_weight=self_key_weight, mixer_output_weight=mixer_output_weight, second_batch_rows=second_batch_rows, routed_expert_index=routed_expert_index, routing_output_weight=routing_output_weight, expert_norm_gain=expert_norm_gain, expert_gate_weight=expert_gate_weight, expert_up_weight=expert_up_weight, expert_down_weight=expert_down_weight, common_expert_gate=common_expert_gate, common_expert_up=common_expert_up, common_expert_down=common_expert_down)


HIGHEST = lax.Precision.HIGHEST
NORM_FLOOR = 1.0

def decay_terms(decay_data_input, correction_rate_input, decay_channel_offset):
    pre_log = -jax.nn.softplus(-(decay_channel_offset + decay_data_input.astype(jnp.float32))) - 0.5
    return (jnp.exp(-jnp.exp(pre_log)), jax.nn.sigmoid(correction_rate_input.astype(jnp.float32)))

def head_view(matrix):
    return matrix.astype(jnp.float32).reshape(matrix.shape[0], -1, HEAD_CHANNELS)

def complete_head_outputs(state_readout, receptance_rows, key_row_block, value_row_block, head_norm_gain, self_key_weight, mixer_output_gate):
    mean_part = lax.optimization_barrier(jnp.mean(state_readout, axis=-1, keepdims=True))
    spread = lax.optimization_barrier(jnp.mean(jnp.square(state_readout - mean_part), axis=-1, keepdims=True))
    normalized_rows = (state_readout - mean_part) * lax.rsqrt(spread + NORM_FLOOR)
    sequence_length = state_readout.shape[0]
    normalized_rows = normalized_rows.reshape(sequence_length, -1) * head_norm_gain
    self_key_term = lax.optimization_barrier(jnp.sum(receptance_rows * key_row_block * self_key_weight.reshape(-1, HEAD_CHANNELS), axis=-1, keepdims=True)) * value_row_block
    mixer_result = (normalized_rows + self_key_term.reshape(sequence_length, -1)) * mixer_output_gate.astype(jnp.float32)
    return mixer_result.astype(jnp.bfloat16)

def token_mixer_baseline(receptance, key_tensor, value_tensor, decay_data_input, correction_rate_input, mixer_output_gate, decay_channel_offset, head_norm_gain, self_key_weight, mixer_output_weight):
    decays, rates = decay_terms(decay_data_input, correction_rate_input, decay_channel_offset)
    receptance_rows = head_view(receptance)
    key_row_block = head_view(key_tensor)
    value_row_block = head_view(value_tensor)
    unit_keys = key_row_block * lax.rsqrt(lax.optimization_barrier(jnp.sum(key_row_block * key_row_block, axis=-1, keepdims=True)) + 1.0)
    decays = decays.reshape(key_row_block.shape)
    rates = rates.reshape(key_row_block.shape)

    def advance(memory, inputs):
        recept_now, decay_now, key_now, value_now, unit_now, rate_now = inputs
        projected = jnp.einsum('hij,hj->hi', memory, unit_now, precision=HIGHEST)
        memory = memory * decay_now[:, None, :] - projected[:, :, None] * (unit_now * rate_now)[:, None, :] + value_now[:, :, None] * key_now[:, None, :]
        return (memory, jnp.einsum('hij,hj->hi', memory, recept_now, precision=HIGHEST))
    head_count = key_row_block.shape[1]
    initial = jnp.zeros((head_count, HEAD_CHANNELS, HEAD_CHANNELS), jnp.float32)
    _, state_readout = lax.scan(advance, initial, (receptance_rows, decays, key_row_block, value_row_block, unit_keys, rates))
    mixer_result = complete_head_outputs(state_readout, receptance_rows, key_row_block, value_row_block, head_norm_gain, self_key_weight, mixer_output_gate)
    groups = mixer_result.reshape(SEQ_MIX, N_TP, MODEL_WIDTH // N_TP).transpose(1, 0, 2)
    weights = mixer_output_weight.reshape(N_TP, MODEL_WIDTH // N_TP, MODEL_WIDTH)

    def add_group(running, blocks):
        mixed_part, weight_part = blocks
        partial_sum = jnp.dot(mixed_part, weight_part, preferred_element_type=jnp.float32).astype(jnp.bfloat16)
        partial_sum = lax.optimization_barrier(partial_sum)
        return (running + partial_sum.astype(jnp.float32), None)
    summed, _ = lax.scan(add_group, jnp.zeros((SEQ_MIX, MODEL_WIDTH), jnp.float32), (groups, weights))
    return summed.astype(jnp.bfloat16)

def expert_unit(rows_in, gate_part, up_part, down_part):
    pre_gate = jnp.dot(rows_in, gate_part.T, preferred_element_type=jnp.float32)
    pre_up = jnp.dot(rows_in, up_part.T, preferred_element_type=jnp.float32)
    hidden = (jax.nn.silu(pre_gate) * pre_up).astype(jnp.bfloat16)
    return jnp.dot(hidden, down_part, preferred_element_type=jnp.float32)

def experts_reference(second_batch_rows, routed_expert_index, routing_output_weight, expert_norm_gain, expert_gate_weight, expert_up_weight, expert_down_weight, common_expert_gate, common_expert_up, common_expert_down):
    widened = second_batch_rows.astype(jnp.float32)
    normalized_rows = (widened * lax.rsqrt(lax.optimization_barrier(jnp.mean(widened * widened, axis=-1, keepdims=True)) + NORM_FLOOR) * expert_norm_gain).astype(jnp.bfloat16)
    shared_out = expert_unit(normalized_rows, common_expert_gate, common_expert_up, common_expert_down)
    flat_ids = routed_expert_index.reshape(-1).astype(jnp.int32)
    ordering = jnp.argsort(flat_ids, stable=True).astype(jnp.int32)
    counts = lax.optimization_barrier(jnp.sum((flat_ids[:, None] == jnp.arange(EXPERTS, dtype=jnp.int32)[None, :]).astype(jnp.int32), axis=0))
    firsts = (jnp.cumsum(counts) - counts).astype(jnp.int32)
    capacity = N_EP * CAP
    padded_order = jnp.concatenate([ordering, jnp.zeros((capacity,), jnp.int32)])
    flat_weights = routing_output_weight.reshape(-1)

    def visit(summed, expert):
        chosen = lax.dynamic_slice_in_dim(padded_order, firsts[expert], capacity)
        usable = jnp.arange(capacity) < counts[expert]
        tokens = chosen // TOP
        copies = expert_unit(normalized_rows[tokens], expert_gate_weight[expert], expert_up_weight[expert], expert_down_weight[expert]).astype(jnp.bfloat16)
        copies = lax.optimization_barrier(copies).astype(jnp.float32)
        factor = jnp.where(usable, flat_weights[chosen], 0.0)
        return (summed.at[tokens].add(copies * factor[:, None]), None)
    routed, _ = lax.scan(visit, jnp.zeros((TOKENS_EXP, MODEL_WIDTH), jnp.float32), jnp.arange(EXPERTS))
    return (routed + shared_out).astype(jnp.bfloat16)

def reference(receptance, key_tensor, value_tensor, decay_data_input, correction_rate_input, mixer_output_gate, decay_channel_offset, head_norm_gain, self_key_weight, mixer_output_weight, second_batch_rows, routed_expert_index, routing_output_weight, expert_norm_gain, expert_gate_weight, expert_up_weight, expert_down_weight, common_expert_gate, common_expert_up, common_expert_down):
    token_mixer_output = token_mixer_baseline(receptance, key_tensor, value_tensor, decay_data_input, correction_rate_input, mixer_output_gate, decay_channel_offset, head_norm_gain, self_key_weight, mixer_output_weight)
    expert_out = experts_reference(second_batch_rows, routed_expert_index, routing_output_weight, expert_norm_gain, expert_gate_weight, expert_up_weight, expert_down_weight, common_expert_gate, common_expert_up, common_expert_down)
    return (token_mixer_output, expert_out)
```

```python
import functools
import math

import jax
import jax.numpy as jnp
from jax import lax
from jax.experimental import pallas as pl
from jax.experimental.pallas import tpu as pltpu
from jax.sharding import PartitionSpec as P

HEAD = 64
SPAN = 64
NORM_FLOOR = 1.0
F32 = jnp.float32
BF = jnp.bfloat16
MESH = pl.DeviceIdType.MESH
DIMS = {
    "nn": (((1,), (0,)), ((), ())),
    "nt": (((1,), (1,)), ((), ())),
    "tn": (((0,), (0,)), ((), ())),
}


def dot(a, b, form="nn"):
    return lax.dot_general(a, b, DIMS[form], preferred_element_type=F32)


def split(x):
    high = x.astype(BF)
    return high, (x - high.astype(F32)).astype(BF)


def spread(x, mask):
    copies = mask.shape[0] // x.shape[0]
    return (x if copies == 1 else jnp.concatenate([x] * copies, axis=0)) * mask


def per_head(a, b, mask, form="nn", fine=False):
    if not fine:
        return dot(a.astype(BF), spread(b.astype(BF), mask), form)
    a_high, a_low = split(a)
    b_high, b_low = split(b)
    rows = a.shape[0]
    both = dot(jnp.concatenate([a_high, a_low], axis=0), spread(b_high, mask), form)
    return both[:rows] + both[rows:] + dot(a_high, spread(b_low, mask), form)


def head_sum(x, mask):
    rows = x.shape[0]
    both = dot(jnp.concatenate(split(x), axis=0), mask)
    return both[:rows] + both[rows:]


def fold(full, mask32):
    full = full * mask32
    out = full[:HEAD]
    for i in range(1, full.shape[0] // HEAD):
        out = out + full[i * HEAD : (i + 1) * HEAD]
    return out


def iotas(rows, lanes):
    at = lax.broadcasted_iota(jnp.int32, (rows, lanes), 0)
    s = lax.broadcasted_iota(jnp.int32, (rows, lanes), 1) & (HEAD - 1)
    return at, s


def local_span(recept, keys, values, data, rate, offset, mask):
    group = recept.shape[1]
    at, s = iotas(SPAN, group)
    recept, keys, values = recept.astype(F32), keys.astype(F32), values.astype(F32)
    step = -math.exp(-0.5) * jax.nn.sigmoid(offset + data.astype(F32))
    row = lax.broadcasted_iota(jnp.int32, (SPAN, SPAN), 0)
    col = lax.broadcasted_iota(jnp.int32, (SPAN, SPAN), 1)
    reach = jnp.where(row >= col, 1.0, 0.0).astype(BF)
    step_high, step_low = split(step)
    total = dot(reach, step_high) + dot(reach, step_low)
    units = keys * lax.rsqrt(head_sum(keys * keys, mask) + 1.0)
    fixes = units * jax.nn.sigmoid(rate.astype(F32))
    last = total[SPAN - 1 : SPAN]
    grown = jnp.exp(-total)
    tail = jnp.exp(last - total)
    unit_in = units * jnp.exp(total - step)
    recept_in = recept * jnp.exp(total)
    zero = jnp.zeros((SPAN, group), F32)
    left = jnp.concatenate([unit_in, recept_in], axis=0)
    key_scores = per_head(left, keys * grown, mask, "nt")
    fix_scores = per_head(left, fixes * grown, mask, "nt")
    unit_key = jnp.where(at > s, key_scores[:SPAN], zero)
    unit_fix = jnp.where(at > s, fix_scores[:SPAN], zero)
    read_key = jnp.where(at >= s, key_scores[SPAN:], zero)
    read_fix = jnp.where(at >= s, fix_scores[SPAN:], zero)
    inverse = None
    for level in range(SPAN.bit_length() - 1):
        pair = (
            ((at >> (level + 1)) == (s >> (level + 1)))
            & (((at >> level) & 1) == 1)
            & (((s >> level) & 1) == 0)
        )
        below = jnp.where(pair, unit_fix, zero)
        if inverse is None:
            inverse = jnp.where(at == s, 1.0, 0.0) - below
        else:
            inverse = inverse - per_head(per_head(inverse, below, mask), inverse, mask)
    key_values = per_head(jnp.concatenate([unit_key, read_key], axis=0), values, mask)
    solved_state = per_head(inverse, unit_in, mask)
    solved_value = per_head(inverse, key_values[:SPAN], mask)
    read_state = recept_in - per_head(read_fix, solved_state, mask)
    read_value = key_values[SPAN:] - per_head(read_fix, solved_value, mask)
    key_tail = (keys * tail).astype(BF)
    fix_tail = (-fixes * tail).astype(BF)
    mask32 = mask.astype(F32)
    move = fold(dot(fix_tail, solved_state.astype(BF), "tn"), mask32)
    move = move + jnp.where(at == s, jnp.exp(last), zero)
    add = fold(
        dot(
            jnp.concatenate([key_tail, fix_tail], axis=0),
            jnp.concatenate([values.astype(BF), solved_value.astype(BF)], axis=0),
            "tn",
        ),
        mask32,
    )
    return read_state, read_value, move, add


def silu(v):
    return v / (1.0 + jnp.exp(-v))


def whole_kernel(
    sizes,
    recept_in, keys_in, values_in, data_in, rate_in, gate_in,
    offset_in, gain_in, self_in, out_weight_in,
    second_in, meta_in, norm_in,
    gate_w_in, up_w_in, down_w_in, common_gate_in, common_up_in, common_down_in,
    token_out, expert_out,
    mix, gate_v, out_w, second, rows, meta, gate_up, down, common, common_d,
    picks, hidden, shared, part, part_in, back, back_in, maps, reads, steps, mixed, mask_v,
    load_s, zs, zr, ms, mr, rs, rr, hs, hr, cs, cr, ps, pr, fs, fr, os, orr, bs, br, ws, wr,
):
    n_z, n_tp, top, cap = sizes
    e = lax.axis_index("ep")
    t = lax.axis_index("tp")
    z = e // 2
    c = e % 2
    positions, width = recept_in.shape
    group = min(256, width)
    groups = width // group
    spans = positions // SPAN
    row_count, model = second_in.shape
    piece = model // n_tp
    hid = common_gate_in.shape[0]

    partner = (e + 1 - 2 * c, t)

    def z_at(d):
        return (z + d) % n_z

    def z_dev(d):
        return (z_at(d) * 2 + c, t)

    def tp_dev(d):
        return (e, (t + d) % n_tp)

    def send(src, dst, ssem, rsem, dev):
        return pltpu.make_async_remote_copy(
            src_ref=src, dst_ref=dst, send_sem=ssem, recv_sem=rsem,
            device_id=dev, device_id_type=MESH,
        )

    def load(src, dst, k):
        return pltpu.make_async_copy(src, dst, load_s.at[k])

    loads = [
        load(second_in, second, 0),
        load(gate_w_in.at[0], gate_up.at[c, pl.ds(0, hid)], 1),
        load(up_w_in.at[0], gate_up.at[c, pl.ds(hid, hid)], 2),
        load(common_gate_in, common.at[pl.ds(0, hid)], 3),
        load(common_up_in, common.at[pl.ds(hid, hid)], 4),
        load(recept_in, mix.at[0], 5),
        load(keys_in, mix.at[1], 6),
        load(values_in, mix.at[2], 7),
        load(data_in, mix.at[3], 8),
        load(rate_in, mix.at[4], 9),
        load(gate_in, gate_v, 10),
        load(down_w_in.at[0], down.at[c], 11),
        load(out_weight_in, out_w, 12),
        load(common_down_in, common_d, 13),
    ]
    for copy in loads:
        copy.start()

    barrier = pltpu.get_barrier_semaphore()
    peers = [partner] + [z_dev(d) for d in range(1, n_z)] + [tp_dev(d) for d in range(1, n_tp)]
    for dev in peers:
        pl.semaphore_signal(barrier, inc=1, device_id=dev, device_id_type=MESH)

    loads[0].wait()
    wide = second[...].astype(F32)
    scale = lax.rsqrt(jnp.mean(wide * wide, axis=-1, keepdims=True) + NORM_FLOOR)
    for k in range(n_tp):
        lanes = pl.ds(k * piece, piece)
        rows[k, z] = (
            second[:, lanes].astype(F32) * scale * norm_in[:, lanes]
        ).astype(BF)
    meta[z] = meta_in[...]
    r_i = lax.broadcasted_iota(jnp.int32, (group, group), 0)
    c_i = lax.broadcasted_iota(jnp.int32, (group, group), 1)
    mask_v[...] = jnp.where((r_i >> 6) == (c_i >> 6), 1.0, 0.0).astype(BF)

    pl.semaphore_wait(barrier, len(peers))

    def rows_z(d):
        return send(rows.at[t, z], rows.at[t, z], zs.at[d], zr.at[d], z_dev(d))

    def rows_z_wait(d):
        w = z_at(n_z - d)
        return send(rows.at[t, w], rows.at[t, w], zs.at[d], zr.at[d], z_dev(d))

    def meta_z(d):
        return send(meta.at[z], meta.at[z], ms.at[d], mr.at[d], z_dev(d))

    def meta_z_wait(d):
        w = z_at(n_z - d)
        return send(meta.at[w], meta.at[w], ms.at[d], mr.at[d], z_dev(d))

    for d in range(1, n_z):
        rows_z(d).start()
    for d in range(1, n_z):
        meta_z(d).start()
    swap = [
        send(gate_w_in.at[0], gate_up.at[c, pl.ds(0, hid)], ws.at[0], wr.at[0], partner),
        send(up_w_in.at[0], gate_up.at[c, pl.ds(hid, hid)], ws.at[1], wr.at[1], partner),
        send(down_w_in.at[0], down.at[c], ws.at[2], wr.at[2], partner),
    ]
    swap_wait = [
        send(gate_w_in.at[0], gate_up.at[1 - c, pl.ds(0, hid)], ws.at[0], wr.at[0], partner),
        send(up_w_in.at[0], gate_up.at[1 - c, pl.ds(hid, hid)], ws.at[1], wr.at[1], partner),
        send(down_w_in.at[0], down.at[1 - c], ws.at[2], wr.at[2], partner),
    ]
    for copy in swap:
        copy.start()

    def both_dots(zz, weight):
        total = None
        for k in range(n_tp):
            term = dot(rows[k, zz], weight[:, k * piece : (k + 1) * piece], "nt")
            total = term if total is None else total + term
        return (silu(total[:, :hid]) * total[:, hid:]).astype(BF)

    def shared_to(d, slot):
        return send(shared.at[slot], shared.at[slot], cs.at[d], cr.at[d], tp_dev(d))

    loads[3].wait()
    loads[4].wait()
    shared[t] = both_dots(z, common)
    for d in range(1, n_tp):
        shared_to(d, t).start()

    def hidden_to(d, k, src):
        zz = z_at(d)
        return send(hidden.at[src, zz], hidden.at[src, zz], hs.at[d, k], hr.at[d, k], tp_dev(k))

    def routes(zz):
        cols = jnp.transpose(meta[zz])
        base = (z * 2).astype(F32)
        return cols, base

    def routed(d):
        zz = z_at(d)
        cols, base = routes(zz)
        lane = lax.broadcasted_iota(jnp.int32, (row_count, 128), 1).astype(F32) + base
        named = jnp.zeros((row_count, 128), F32)
        for k in range(top):
            named = named + jnp.where(cols[:, k : k + 1] == lane, 1.0, 0.0)
        row = lax.broadcasted_iota(jnp.int32, (row_count, row_count), 0)
        col = lax.broadcasted_iota(jnp.int32, (row_count, row_count), 1)
        rank = dot(jnp.where(row > col, 1.0, 0.0).astype(BF), named.astype(BF))
        slot = lax.broadcasted_iota(jnp.int32, (row_count, cap), 1).astype(F32)
        for x in range(2):
            pick = jnp.where(
                slot == rank[:, x : x + 1],
                jnp.broadcast_to(named[:, x : x + 1], (row_count, cap)),
                0.0,
            ).astype(BF)
            picks[zz, x] = pick
            units = both_dots(zz, gate_up[x])
            hidden[t, zz, pl.ds(x * cap, cap)] = dot(pick, units, "tn").astype(BF)
        for k in range(1, n_tp):
            hidden_to(d, k, t).start()

    loads[1].wait()
    loads[2].wait()
    swap_wait[0].wait_recv()
    swap_wait[1].wait_recv()
    routed(0)

    def relay_to(d, k, src):
        zz = z_at(d)
        return send(rows.at[src, zz], rows.at[src, zz], rs.at[d, k], rr.at[d, k], tp_dev(k))

    def relay(d):
        rows_z_wait(n_z - d).wait_recv()
        for k in range(1, n_tp):
            relay_to(d, k, t).start()

    for copy in loads[5:10]:
        copy.wait()
    per_step = -(-(n_z - 1) // spans)

    def span_step(b, carry):
        span = pl.ds(b * SPAN, SPAN)
        for g in range(groups):
            lanes = pl.ds(g * group, group)
            read_state, read_value, move, add = local_span(
                mix[0, span, lanes], mix[1, span, lanes], mix[2, span, lanes],
                mix[3, span, lanes], mix[4, span, lanes], offset_in[:, lanes], mask_v[...],
            )
            reads[0, span, lanes] = read_state
            reads[1, span, lanes] = read_value
            steps[0, b, :, lanes] = move
            steps[1, b, :, lanes] = add
        for i in range(per_step):
            d = b * per_step + i + 1

            @pl.when(d < n_z)
            def _():
                relay(d)

        return carry

    lax.fori_loop(0, spans, span_step, 0)

    for g in range(groups):
        lanes = pl.ds(g * group, group)
        mask = mask_v[...]
        move, add = steps[0, 0, :, lanes], steps[1, 0, :, lanes]
        for b in range(1, spans):
            here = steps[0, b, :, lanes]
            move, add = (
                per_head(here, move, mask, fine=True),
                per_head(here, add, mask, fine=True) + steps[1, b, :, lanes],
            )
        maps[z, c, :, lanes] = move.astype(BF)
        maps[z, c, :, pl.ds(width + g * group, group)] = add.astype(BF)

    def map_z(d):
        return send(maps.at[z, c], maps.at[z, c], ps.at[d], pr.at[d], z_dev(d))

    def map_z_wait(d):
        w = z_at(n_z - d)
        return send(maps.at[w, c], maps.at[w, c], ps.at[d], pr.at[d], z_dev(d))

    def map_on(d, core):
        w = z_at(n_z - d)
        return send(maps.at[w, core], maps.at[w, core], fs.at[d], fr.at[d], partner)

    for d in range(1, n_z):
        map_z(d).start()
    map_on(0, c).start()

    def routed_step(d, carry):
        meta_z_wait(n_z - d).wait_recv()
        for k in range(1, n_tp):
            relay_to(d, k, (t - k + n_tp) % n_tp).wait_recv()
        routed(d)
        return carry

    lax.fori_loop(1, n_z, routed_step, 0)

    for d in range(1, n_z):
        map_z_wait(d).wait_recv()
        map_on(d, c).start()
    for d in range(n_z):
        map_on(d, 1 - c).wait_recv()

    def prefix(i, state):
        both = maps[i // 2, i % 2]
        out = []
        for g in range(groups):
            lanes = slice(g * group, (g + 1) * group)
            after = slice(width + g * group, width + (g + 1) * group)
            out.append(
                per_head(both[:, lanes].astype(F32), state[:, lanes], mask_v[...], fine=True)
                + both[:, after].astype(F32)
            )
        return jnp.concatenate(out, axis=1) if groups > 1 else out[0]

    state = lax.fori_loop(0, e, prefix, jnp.zeros((HEAD, width), F32))

    loads[10].wait()

    def finish_step(b, state):
        span = pl.ds(b * SPAN, SPAN)
        following = []
        for g in range(groups):
            lanes = pl.ds(g * group, group)
            mask = mask_v[...]
            both = per_head(
                jnp.concatenate([reads[0, span, lanes], steps[0, b, :, lanes]], axis=0),
                state[:, g * group : (g + 1) * group],
                mask,
                fine=True,
            )
            following.append(both[SPAN:] + steps[1, b, :, lanes])
            read = reads[1, span, lanes] + both[:SPAN]
            recept, keys = mix[0, span, lanes].astype(F32), mix[1, span, lanes].astype(F32)
            sums = head_sum(
                jnp.concatenate([read, recept * keys * self_in[:, lanes]], axis=0), mask
            )
            apart = read - sums[:SPAN] * (1.0 / HEAD)
            spread_sum = head_sum(apart * apart, mask) * (1.0 / HEAD)
            normed = apart * lax.rsqrt(spread_sum + NORM_FLOOR) * gain_in[:, lanes]
            out = (normed + sums[SPAN:] * mix[2, span, lanes].astype(F32)) * gate_v[
                span, lanes
            ].astype(F32)
            mixed[span, lanes] = out.astype(BF)
        return jnp.concatenate(following, axis=1) if groups > 1 else following[0]

    lax.fori_loop(0, spans, finish_step, state)

    loads[12].wait()
    share = positions // n_tp
    wide_cols = min(512, model)

    def project(i, carry):
        lanes = pl.ds(pl.multiple_of(i * wide_cols, 128), wide_cols)
        got = dot(mixed[...], out_w[:, lanes]).astype(BF)
        for k in range(n_tp):
            part[k, :, lanes] = got[k * share : (k + 1) * share]
        return carry

    lax.fori_loop(0, model // wide_cols, project, 0)

    def part_to(d):
        return send(
            part.at[(t + d) % n_tp], part_in.at[d], os.at[d], orr.at[d], tp_dev(d)
        )

    for d in range(1, n_tp):
        part_to(d).start()

    loads[11].wait()
    swap_wait[2].wait_recv()

    def back_to(d):
        return send(back.at[z_at(d)], back_in.at[d], bs.at[d], br.at[d], z_dev(d))

    def routed_out(d):
        zz = z_at(d)
        cols, base = routes(zz)
        for k in range(1, n_tp):
            hidden_to(d, k, (t - k + n_tp) % n_tp).wait_recv()
        total = None
        for x in range(2):
            copies = None
            for k in range(n_tp):
                term = dot(
                    hidden[k, zz, pl.ds(x * cap, cap)], down[x, pl.ds(k * hid, hid)]
                )
                copies = term if copies is None else copies + term
            factor = jnp.zeros((row_count, 1), F32)
            for k in range(top):
                factor = factor + jnp.where(
                    cols[:, k : k + 1] == base + float(x), cols[:, top + k : top + k + 1], 0.0
                )
            term = dot(picks[zz, x], copies.astype(BF)) * factor
            total = term if total is None else total + term
        return total

    def back_step(d, carry):
        back[z_at(d)] = routed_out(d).astype(BF)
        back_to(d).start()
        return carry

    lax.fori_loop(1, n_z, back_step, 0)
    result = routed_out(0)

    loads[13].wait()
    for d in range(1, n_tp):
        shared_to(d, (t - d + n_tp) % n_tp).wait_recv()
    for k in range(n_tp):
        result = result + dot(shared[k], common_d[pl.ds(k * hid, hid)])

    for d in range(1, n_tp):
        part_to(d).wait_recv()
    summed = part[t].astype(F32)
    for d in range(1, n_tp):
        summed = summed + part_in[d].astype(F32)
    token_out[...] = summed.astype(BF)

    for d in range(1, n_z):
        back_to(d).wait_recv()
    for d in range(1, n_z):
        result = result + back_in[d].astype(F32)
    expert_out[...] = result.astype(BF)

    for copy in swap:
        copy.wait_send()
    for d in range(1, n_z):
        rows_z(d).wait_send()
        meta_z(d).wait_send()
        map_z(d).wait_send()
        back_to(d).wait_send()
    for d in range(n_z):
        map_on(d, c).wait_send()
        for k in range(1, n_tp):
            hidden_to(d, k, t).wait_send()
            if d:
                relay_to(d, k, t).wait_send()
    for k in range(1, n_tp):
        shared_to(k, t).wait_send()
        part_to(k).wait_send()


def on_device(n_ep, n_tp, *args):
    (
        receptance, key_tensor, value_tensor, decay_data_input, correction_rate_input,
        mixer_output_gate, decay_channel_offset, head_norm_gain, self_key_weight,
        mixer_output_weight, second_batch_rows, routed_expert_index, routing_output_weight,
        expert_norm_gain, expert_gate_weight, expert_up_weight, expert_down_weight,
        common_expert_gate, common_expert_up, common_expert_down,
    ) = args
    n_z = n_ep // 2
    positions, width = receptance.shape
    row_count, model = second_batch_rows.shape
    top = routed_expert_index.shape[1]
    cap = 3 * row_count * top // (2 * n_ep)
    cap = -(-cap // 16) * 16
    hid = common_expert_gate.shape[0]
    units = common_expert_down.shape[0]
    piece = model // n_tp
    group = min(256, width)
    spans = positions // SPAN
    meta = jnp.concatenate(
        [routed_expert_index.T.astype(F32), routing_output_weight.T], axis=0
    )
    any_spec = pl.BlockSpec(memory_space=pl.ANY)
    vmem = pl.BlockSpec(memory_space=pltpu.VMEM)
    dma = pltpu.SemaphoreType.DMA
    share = positions // n_tp
    return pl.pallas_call(
        functools.partial(whole_kernel, (n_z, n_tp, top, cap)),
        out_shape=(
            jax.ShapeDtypeStruct((share, model), BF),
            jax.ShapeDtypeStruct((row_count, piece), BF),
        ),
        in_specs=[any_spec] * 6 + [vmem] * 3 + [any_spec] + [any_spec, vmem, vmem] + [any_spec] * 6,
        out_specs=(vmem, vmem),
        scratch_shapes=[
            pltpu.VMEM((5, positions, width), BF),
            pltpu.VMEM((positions, width), BF),
            pltpu.VMEM((width, model), BF),
            pltpu.VMEM((row_count, model), BF),
            pltpu.VMEM((n_tp, n_z, row_count, piece), BF),
            pltpu.VMEM((n_z, 2 * top, row_count), F32),
            pltpu.VMEM((2, 2 * hid, model), BF),
            pltpu.VMEM((2, units, piece), BF),
            pltpu.VMEM((2 * hid, model), BF),
            pltpu.VMEM((units, piece), BF),
            pltpu.VMEM((n_z, 2, row_count, cap), BF),
            pltpu.VMEM((n_tp, n_z, 2 * cap, hid), BF),
            pltpu.VMEM((n_tp, row_count, hid), BF),
            pltpu.VMEM((n_tp, share, model), BF),
            pltpu.VMEM((n_tp, share, model), BF),
            pltpu.VMEM((n_z, row_count, piece), BF),
            pltpu.VMEM((n_z, row_count, piece), BF),
            pltpu.VMEM((n_z, 2, HEAD, 2 * width), BF),
            pltpu.VMEM((2, positions, width), F32),
            pltpu.VMEM((2, spans, HEAD, width), F32),
            pltpu.VMEM((positions, width), BF),
            pltpu.VMEM((group, group), BF),
            dma((14,)),
            dma((n_z,)), dma((n_z,)), dma((n_z,)), dma((n_z,)),
            dma((n_z, n_tp)), dma((n_z, n_tp)), dma((n_z, n_tp)), dma((n_z, n_tp)),
            dma((n_tp,)), dma((n_tp,)),
            dma((n_z,)), dma((n_z,)), dma((n_z,)), dma((n_z,)),
            dma((n_tp,)), dma((n_tp,)),
            dma((n_z,)), dma((n_z,)),
            dma((3,)), dma((3,)),
        ],
        compiler_params=pltpu.CompilerParams(
            collective_id=0, has_side_effects=True, vmem_limit_bytes=60 * 1024 * 1024
        ),
        name="mixer_and_experts",
    )(
        receptance, key_tensor, value_tensor, decay_data_input, correction_rate_input,
        mixer_output_gate, decay_channel_offset[None], head_norm_gain[None],
        self_key_weight[None], mixer_output_weight, second_batch_rows, meta,
        expert_norm_gain[None], expert_gate_weight, expert_up_weight, expert_down_weight,
        common_expert_gate, common_expert_up, common_expert_down,
    )


def solution(mesh):
    in_specs = (
        (P("ep", "tp"),) * 6
        + (P("tp"),) * 3
        + (P("tp", None),)
        + (P("ep", None),) * 3
        + (P(), P("ep", "tp", None), P("ep", "tp", None), P("ep", None, "tp"))
        + (P("tp", None), P("tp", None), P(None, "tp"))
    )
    out_specs = (P(("ep", "tp"), None), P("ep", "tp"))
    return jax.shard_map(
        functools.partial(on_device, mesh.shape["ep"], mesh.shape["tp"]),
        mesh=mesh, in_specs=in_specs, out_specs=out_specs, check_vma=False,
    )
```

```python
import functools
import math

import jax
import jax.numpy as jnp
from jax import lax
from jax.experimental import pallas as pl
from jax.experimental.pallas import tpu as pltpu
from jax.sharding import PartitionSpec as P

HEAD = 64
SPAN = 64
SPANS_AT_ONCE = 2
NORM_FLOOR = 1.0
F32 = jnp.float32
BF = jnp.bfloat16
MESH = pl.DeviceIdType.MESH
DIMS = {
    "nn": (((1,), (0,)), ((), ())),
    "nt": (((1,), (1,)), ((), ())),
    "tn": (((0,), (0,)), ((), ())),
}


def dot(a, b, form="nn"):
    return lax.dot_general(a, b, DIMS[form], preferred_element_type=F32)


def split(x):
    high = x.astype(BF)
    return high, (x - high.astype(F32)).astype(BF)


def spread(x, mask):
    lanes = min(128, x.shape[1])
    tiles = x.shape[1] // lanes
    none = jnp.zeros((lanes, lanes), x.dtype)
    columns = []
    for j in range(tiles):
        piece = x[:, j * lanes : (j + 1) * lanes]
        block = jnp.concatenate([piece] * (lanes // HEAD), axis=0) * mask
        columns.append(jnp.concatenate([none] * j + [block] + [none] * (tiles - 1 - j), axis=0))
    return columns[0] if tiles == 1 else jnp.concatenate(columns, axis=1)


def per_head(a, b, mask, form="nn", fine=False):
    return per_heads([a], [b], mask, form, fine)[0]


def per_heads(lefts, rights, mask, form="nn", fine=False):
    if not fine:
        return [
            dot(a.astype(BF), spread(b.astype(BF), mask), form) for a, b in zip(lefts, rights)
        ]
    lefts, rights = [split(a) for a in lefts], [split(b) for b in rights]
    both = [
        dot(jnp.concatenate(a, axis=0), spread(b[0], mask), form) for a, b in zip(lefts, rights)
    ]
    rest = [dot(a[0], spread(b[1], mask), form) for a, b in zip(lefts, rights)]
    rows = lefts[0][0].shape[0]
    return [x[:rows] + x[rows:] + y for x, y in zip(both, rest)]


def head_sums(xs, ones):
    rows = xs[0].shape[0]
    both = [dot(jnp.concatenate(split(x), axis=0), ones) for x in xs]
    return [x[:rows] + x[rows:] for x in both]


def fold(full):
    lanes = min(128, full.shape[1])
    low = lax.broadcasted_iota(jnp.int32, (HEAD, lanes), 1) < HEAD
    out = []
    for j in range(full.shape[1] // lanes):
        block = full[:, j * lanes : (j + 1) * lanes]
        at = j * lanes
        out.append(
            jnp.where(low, block[at : at + HEAD], block[at + HEAD : at + 2 * HEAD])
            if lanes > HEAD
            else block[at : at + HEAD]
        )
    return out[0] if len(out) == 1 else jnp.concatenate(out, axis=1)


def iotas(rows, lanes):
    at = lax.broadcasted_iota(jnp.int32, (rows, lanes), 0)
    s = lax.broadcasted_iota(jnp.int32, (rows, lanes), 1) & (HEAD - 1)
    return at, s


def local_spans(problems, mask, ones):
    group = problems[0][0].shape[1]
    at, s = iotas(SPAN, group)
    zero = jnp.zeros((SPAN, group), F32)
    row = lax.broadcasted_iota(jnp.int32, (SPAN, SPAN), 0)
    col = lax.broadcasted_iota(jnp.int32, (SPAN, SPAN), 1)
    reach = jnp.where(row >= col, 1.0, 0.0).astype(BF)
    many = range(len(problems))
    recepts = [p[0].astype(F32) for p in problems]
    keys = [p[1].astype(F32) for p in problems]
    values = [p[2] for p in problems]
    step = [-math.exp(-0.5) * jax.nn.sigmoid(p[5] + p[3].astype(F32)) for p in problems]
    parts = [split(x) for x in step]
    high = [dot(reach, x[0]) for x in parts]
    low = [dot(reach, x[1]) for x in parts]
    total = [x + y for x, y in zip(high, low)]
    squares = head_sums([k * k for k in keys], ones)
    units = [k * lax.rsqrt(q + 1.0) for k, q in zip(keys, squares)]
    fixes = [u * jax.nn.sigmoid(p[4].astype(F32)) for u, p in zip(units, problems)]
    grown = [jnp.exp(-x) for x in total]
    unit_in = [units[i] * jnp.exp(total[i] - step[i]) for i in many]
    recept_in = [recepts[i] * jnp.exp(total[i]) for i in many]
    left = [jnp.concatenate([unit_in[i], recept_in[i]], axis=0) for i in many]
    fix_scores = per_heads(left, [fixes[i] * grown[i] for i in many], mask, "nt")
    key_scores = per_heads(left, [keys[i] * grown[i] for i in many], mask, "nt")
    unit_fix = [jnp.where(at > s, x[:SPAN], zero) for x in fix_scores]
    read_fix = [jnp.where(at >= s, x[SPAN:], zero) for x in fix_scores]
    both_key = [
        jnp.concatenate(
            [jnp.where(at > s, x[:SPAN], zero), jnp.where(at >= s, x[SPAN:], zero)], axis=0
        )
        for x in key_scores
    ]
    key_values = per_heads(both_key, values, mask)
    inverse = None
    for level in range(SPAN.bit_length() - 1):
        pair = (
            ((at >> (level + 1)) == (s >> (level + 1)))
            & (((at >> level) & 1) == 1)
            & (((s >> level) & 1) == 0)
        )
        below = [jnp.where(pair, x, zero) for x in unit_fix]
        if inverse is None:
            inverse = [jnp.where(at == s, 1.0, 0.0) - x for x in below]
        else:
            first = per_heads(inverse, below, mask)
            second = per_heads(first, inverse, mask)
            inverse = [x - y for x, y in zip(inverse, second)]
    solved_state = per_heads(inverse, unit_in, mask)
    solved_value = per_heads(inverse, [x[:SPAN] for x in key_values], mask)
    from_state = per_heads(read_fix, solved_state, mask)
    from_value = per_heads(read_fix, solved_value, mask)
    last = [x[SPAN - 1 : SPAN] for x in total]
    tail = [jnp.exp(last[i] - total[i]) for i in many]
    fix_tail = [(-fixes[i] * tail[i]).astype(BF) for i in many]
    key_tail = [(keys[i] * tail[i]).astype(BF) for i in many]
    moves = [dot(fix_tail[i], solved_state[i].astype(BF), "tn") for i in many]
    adds = [
        dot(
            jnp.concatenate([key_tail[i], fix_tail[i]], axis=0),
            jnp.concatenate([values[i], solved_value[i].astype(BF)], axis=0),
            "tn",
        )
        for i in many
    ]
    return [
        (
            recept_in[i] - from_state[i],
            key_values[i][SPAN:] - from_value[i],
            fold(moves[i]) + jnp.where(at == s, jnp.exp(last[i]), zero),
            fold(adds[i]),
        )
        for i in many
    ]


def silu(v):
    return v / (1.0 + jnp.exp(-v))


def whole_kernel(
    sizes,
    recept_in, keys_in, values_in, data_in, rate_in, gate_in,
    offset_in, gain_in, self_in, out_weight_in,
    second_in, ids_in, factor_in, norm_in,
    gate_w_in, up_w_in, down_w_in, common_gate_in, common_up_in, common_down_in,
    token_out, expert_out,
    mix, gate_v, out_w, second, rows, meta, gate_up, down, common, common_d,
    picks, hidden, shared, part, part_in, back, back_in, maps, reads, steps, mixed, mask_v,
    load_s, zs, zr, ms, mr, rs, rr, hs, hr, cs, cr, ps, pr, fs, fr, os, orr, bs, br, ws, wr,
):
    n_z, n_tp, top, cap = sizes
    e = lax.axis_index("ep")
    t = lax.axis_index("tp")
    z = e // 2
    c = e % 2
    positions, width = recept_in.shape
    group = min(256, width)
    groups = width // group
    lane_tile = min(128, group)
    spans = positions // SPAN
    row_count, model = second_in.shape
    piece = model // n_tp
    hid = common_gate_in.shape[0]

    partner = (e + 1 - 2 * c, t)

    def z_at(d):
        return (z + d) % n_z

    def z_dev(d):
        return (z_at(d) * 2 + c, t)

    def tp_dev(d):
        return (e, (t + d) % n_tp)

    def send(src, dst, ssem, rsem, dev):
        return pltpu.make_async_remote_copy(
            src_ref=src, dst_ref=dst, send_sem=ssem, recv_sem=rsem,
            device_id=dev, device_id_type=MESH,
        )

    def load(src, dst, k):
        return pltpu.make_async_copy(src, dst, load_s.at[k])

    loads = [
        load(second_in, second, 0),
        load(common_gate_in, common.at[pl.ds(0, hid)], 1),
        load(common_up_in, common.at[pl.ds(hid, hid)], 2),
        load(gate_w_in.at[0], gate_up.at[c, pl.ds(0, hid)], 3),
        load(up_w_in.at[0], gate_up.at[c, pl.ds(hid, hid)], 4),
        load(recept_in, mix.at[0], 5),
        load(keys_in, mix.at[1], 6),
        load(values_in, mix.at[2], 7),
        load(data_in, mix.at[3], 8),
        load(rate_in, mix.at[4], 9),
        load(gate_in, gate_v, 10),
        load(down_w_in.at[0], down.at[c], 11),
        load(out_weight_in, out_w, 12),
        load(common_down_in, common_d, 13),
    ]
    loads[0].start()

    barrier = pltpu.get_barrier_semaphore()
    peers = [partner] + [z_dev(d) for d in range(1, n_z)] + [tp_dev(d) for d in range(1, n_tp)]
    for dev in peers:
        pl.semaphore_signal(barrier, inc=1, device_id=dev, device_id_type=MESH)
    for copy in loads[1:5]:
        copy.start()

    r_i = lax.broadcasted_iota(jnp.int32, (group, group), 0)
    c_i = lax.broadcasted_iota(jnp.int32, (group, group), 1)
    mask_v[...] = jnp.where((r_i >> 6) == (c_i >> 6), 1.0, 0.0).astype(BF)
    meta[z] = jnp.concatenate([ids_in[...].astype(F32), factor_in[...]], axis=0)
    loads[0].wait()
    wide = second[...].astype(F32)
    scale = lax.rsqrt(jnp.mean(wide * wide, axis=-1, keepdims=True) + NORM_FLOOR)
    for k in range(n_tp):
        lanes = pl.ds(k * piece, piece)
        rows[k, z] = (
            second[:, lanes].astype(F32) * scale * norm_in[:, lanes]
        ).astype(BF)
    for copy in loads[5:]:
        copy.start()

    pl.semaphore_wait(barrier, len(peers))

    def rows_z(d):
        return send(rows.at[t, z], rows.at[t, z], zs.at[d], zr.at[d], z_dev(d))

    def rows_z_wait(d):
        w = z_at(n_z - d)
        return send(rows.at[t, w], rows.at[t, w], zs.at[d], zr.at[d], z_dev(d))

    def meta_z(d):
        return send(meta.at[z], meta.at[z], ms.at[d], mr.at[d], z_dev(d))

    def meta_z_wait(d):
        w = z_at(n_z - d)
        return send(meta.at[w], meta.at[w], ms.at[d], mr.at[d], z_dev(d))

    for d in range(1, n_z):
        rows_z(d).start()
    for d in range(1, n_z):
        meta_z(d).start()
    for copy in loads[3:5]:
        copy.wait()
    swap_up = send(gate_up.at[c], gate_up.at[c], ws.at[0], wr.at[0], partner)
    swap_up_in = send(gate_up.at[1 - c], gate_up.at[1 - c], ws.at[0], wr.at[0], partner)
    swap_down = send(down.at[c], down.at[c], ws.at[1], wr.at[1], partner)
    swap_down_in = send(down.at[1 - c], down.at[1 - c], ws.at[1], wr.at[1], partner)
    swap_up.start()

    square = n_tp == 4
    if square:
        x_t, y_t, far_t = t + 1 - 2 * (t % 2), (t + 2) % 4, 3 - t
        x_dev, y_dev = (e, x_t), (e, y_t)

    class Exchange:
        def __init__(self, whole, half, sem_s, sem_r):
            self.whole, self.half, self.sem_s, self.sem_r = whole, half, sem_s, sem_r

        def copy(self, ref, k, dev):
            return send(ref, ref, self.sem_s(k), self.sem_r(k), dev)

        def first(self):
            if square:
                return [self.copy(self.whole(t), 1, x_dev), self.copy(self.whole(t), 2, y_dev)]
            return [self.copy(self.whole(t), k, tp_dev(k)) for k in range(1, n_tp)]

        def second(self):
            if square:
                return [
                    self.copy(self.half(x_t, 0), 3, y_dev),
                    self.copy(self.half(y_t, 1), 0, x_dev),
                ]
            return []

        def start(self):
            for copy in self.first():
                copy.start()

        def forward(self):
            if square:
                ahead = [self.copy(self.whole(x_t), 1, x_dev), self.copy(self.whole(y_t), 2, y_dev)]
                for came, copy in zip(ahead, self.second()):
                    came.wait_recv()
                    copy.start()

        def finish(self):
            if square:
                self.copy(self.half(far_t, 0), 3, y_dev).wait_recv()
                self.copy(self.half(far_t, 1), 0, x_dev).wait_recv()
            else:
                for k in range(1, n_tp):
                    src = (t - k + n_tp) % n_tp
                    self.copy(self.whole(src), k, tp_dev(k)).wait_recv()

        def sent(self):
            for copy in self.first() + self.second():
                copy.wait_send()

    half_rows = row_count // 2
    shared_x = Exchange(
        lambda src: shared.at[src],
        lambda src, i: shared.at[src, pl.ds(i * half_rows, half_rows)],
        lambda k: cs.at[k], lambda k: cr.at[k],
    )

    def rows_x(d):
        zz = z_at(d)
        return Exchange(
            lambda src: rows.at[src, zz],
            lambda src, i: rows.at[src, zz, pl.ds(i * half_rows, half_rows)],
            lambda k: rs.at[d, k], lambda k: rr.at[d, k],
        )

    def hidden_x(d):
        zz = z_at(d)
        return Exchange(
            lambda src: hidden.at[src, zz],
            lambda src, i: hidden.at[src, zz, pl.ds(i * cap, cap)],
            lambda k: hs.at[d, k], lambda k: hr.at[d, k],
        )

    def each(low, high, step):
        if high - low <= 4:
            for d in range(low, high):
                step(d)
        else:
            def body(d, carry):
                step(d)
                return carry

            lax.fori_loop(low, high, body, 0)

    def both_dots(zz, weights):
        totals = [None] * len(weights)
        for i, weight in enumerate(weights):
            for k in range(n_tp):
                term = dot(rows[k, zz], weight[:, k * piece : (k + 1) * piece], "nt")
                totals[i] = term if totals[i] is None else totals[i] + term
        return [(silu(total[:, :hid]) * total[:, hid:]).astype(BF) for total in totals]

    for copy in loads[1:3]:
        copy.wait()
    shared[t] = both_dots(z, [common])[0]
    shared_x.start()

    def routes(zz):
        cols = jnp.transpose(meta[zz])
        base = (z * 2).astype(F32)
        return cols, base

    def routed(d):
        zz = z_at(d)
        cols, base = routes(zz)
        lane = lax.broadcasted_iota(jnp.int32, (row_count, 128), 1).astype(F32) + base
        named = jnp.zeros((row_count, 128), F32)
        for k in range(top):
            named = named + jnp.where(cols[:, k : k + 1] == lane, 1.0, 0.0)
        row = lax.broadcasted_iota(jnp.int32, (row_count, row_count), 0)
        col = lax.broadcasted_iota(jnp.int32, (row_count, row_count), 1)
        rank = dot(jnp.where(row > col, 1.0, 0.0).astype(BF), named.astype(BF))
        slot = lax.broadcasted_iota(jnp.int32, (row_count, cap), 1).astype(F32)
        units = both_dots(zz, [gate_up[0], gate_up[1]])
        chosen = [
            jnp.where(
                slot == rank[:, x : x + 1],
                jnp.broadcast_to(named[:, x : x + 1], (row_count, cap)),
                0.0,
            ).astype(BF)
            for x in range(2)
        ]
        packed = [dot(chosen[x], units[x], "tn").astype(BF) for x in range(2)]
        for x in range(2):
            picks[zz, x] = chosen[x]
            hidden[t, zz, pl.ds(x * cap, cap)] = packed[x]
        hidden_x(d).start()

    def relay(d):
        rows_z_wait(n_z - d).wait_recv()
        rows_x(d).start()

    stride = SPANS_AT_ONCE if spans % SPANS_AT_ONCE == 0 else 1

    def span_step(i):
        where = [
            (i * stride + j, pl.ds((i * stride + j) * SPAN, SPAN), pl.ds(g * group, group))
            for j in range(stride)
            for g in range(groups)
        ]
        found = local_spans(
            [
                tuple(mix[k, span, lanes] for k in range(5)) + (offset_in[:, lanes],)
                for _, span, lanes in where
            ],
            mask_v[:lane_tile, :lane_tile],
            mask_v[...],
        )
        for (b, span, lanes), (read_state, read_value, move, add) in zip(where, found):
            reads[0, span, lanes] = read_state
            reads[1, span, lanes] = read_value
            steps[0, b, :, lanes] = move
            steps[1, b, :, lanes] = add

    for copy in loads[5:10]:
        copy.wait()
    span_step(0)
    swap_up_in.wait_recv()
    routed(0)
    shared_x.forward()
    loads[11].wait()
    swap_down.start()
    each(1, min(3, n_z), relay)
    for i in range(1, spans // stride):
        span_step(i)
    hidden_x(0).forward()
    rows_x(1).forward()
    each(3, n_z, relay)

    tiles = [pl.ds(g * group, group) for g in range(groups)]
    mask = mask_v[:lane_tile, :lane_tile]
    now = [steps[0, 0, :, lanes] for lanes in tiles] + [steps[1, 0, :, lanes] for lanes in tiles]
    for b in range(1, spans):
        now = per_heads([steps[0, b, :, lanes] for lanes in tiles] * 2, now, mask, fine=True)
        for g, lanes in enumerate(tiles):
            now[groups + g] = now[groups + g] + steps[1, b, :, lanes]
    for k in range(2 * groups):
        maps[z, c, :, pl.ds(k * group, group)] = now[k].astype(BF)

    def map_z(d):
        return send(maps.at[z, c], maps.at[z, c], ps.at[d], pr.at[d], z_dev(d))

    def map_z_wait(d):
        w = z_at(n_z - d)
        return send(maps.at[w, c], maps.at[w, c], ps.at[d], pr.at[d], z_dev(d))

    def map_on(d, core):
        w = z_at(n_z - d)
        return send(maps.at[w, core], maps.at[w, core], fs.at[d], fr.at[d], partner)

    for d in range(1, n_z):
        map_z(d).start()
    map_on(0, c).start()

    def routed_step(d):
        meta_z_wait(n_z - d).wait_recv()
        if not isinstance(d, int):
            pl.when(d > 1)(lambda: rows_x(d).forward())
        elif d + 1 < n_z:
            rows_x(d + 1).forward()
        rows_x(d).finish()
        routed(d)
        if isinstance(d, int) and d > 1:
            hidden_x(d - 1).forward()

    each(1, n_z, routed_step)

    for d in range(1, n_z):
        map_z_wait(d).wait_recv()
        map_on(d, c).start()
    if n_z <= 5:
        hidden_x(n_z - 1).forward()
    for d in range(n_z):
        map_on(d, 1 - c).wait_recv()

    def prefix(i, state):
        both = maps[i // 2, i % 2]
        mask = mask_v[:lane_tile, :lane_tile]
        new = per_heads(
            [both[:, g * group : (g + 1) * group].astype(F32) for g in range(groups)],
            state, mask, fine=True,
        )
        return [
            new[g] + both[:, width + g * group : width + (g + 1) * group].astype(F32)
            for g in range(groups)
        ]

    state = lax.fori_loop(
        0, e, prefix, [jnp.zeros((HEAD, group), F32) for _ in range(groups)]
    )

    loads[10].wait()

    def finish_step(b, state):
        span = pl.ds(b * SPAN, SPAN)
        mask, ones = mask_v[:lane_tile, :lane_tile], mask_v[...]
        many = range(groups)
        recepts = [mix[0, span, lanes].astype(F32) for lanes in tiles]
        keys = [mix[1, span, lanes].astype(F32) for lanes in tiles]
        own = [recepts[g] * keys[g] * self_in[:, tiles[g]] for g in many]
        both = per_heads(
            [
                jnp.concatenate([reads[0, span, lanes], steps[0, b, :, lanes]], axis=0)
                for lanes in tiles
            ],
            state, mask, fine=True,
        )
        following = [both[g][SPAN:] + steps[1, b, :, tiles[g]] for g in many]
        read = [reads[1, span, tiles[g]] + both[g][:SPAN] for g in many]
        sums = head_sums([jnp.concatenate([read[g], own[g]], axis=0) for g in many], ones)
        apart = [read[g] - sums[g][:SPAN] * (1.0 / HEAD) for g in many]
        squares = head_sums([x * x for x in apart], ones)
        for g, lanes in enumerate(tiles):
            normed = (
                apart[g] * lax.rsqrt(squares[g] * (1.0 / HEAD) + NORM_FLOOR) * gain_in[:, lanes]
            )
            out = (normed + sums[g][SPAN:] * mix[2, span, lanes].astype(F32)) * gate_v[
                span, lanes
            ].astype(F32)
            mixed[span, lanes] = out.astype(BF)
        return following

    lax.fori_loop(0, spans, finish_step, state)

    loads[12].wait()
    share = positions // n_tp
    wide_cols = min(512, model)

    def project(i, carry):
        lanes = pl.ds(pl.multiple_of(i * wide_cols, 128), wide_cols)
        got = dot(mixed[...], out_w[:, lanes]).astype(BF)
        for k in range(n_tp):
            part[k, :, lanes] = got[k * share : (k + 1) * share]
        return carry

    lax.fori_loop(0, model // wide_cols, project, 0)

    def part_to(d):
        return send(
            part.at[(t + d) % n_tp], part_in.at[d], os.at[d], orr.at[d], tp_dev(d)
        )

    for d in range(1, n_tp):
        part_to(d).start()

    swap_down_in.wait_recv()

    def back_to(d):
        return send(back.at[z_at(d)], back_in.at[d], bs.at[d], br.at[d], z_dev(d))

    def routed_out(d):
        zz = z_at(d)
        cols, base = routes(zz)
        hidden_x(d).finish()
        copies = [None, None]
        for x in range(2):
            for k in range(n_tp):
                term = dot(
                    hidden[k, zz, pl.ds(x * cap, cap)], down[x, pl.ds(k * hid, hid)]
                )
                copies[x] = term if copies[x] is None else copies[x] + term
        terms = [dot(picks[zz, x], copies[x].astype(BF)) for x in range(2)]
        total = None
        for x in range(2):
            factor = jnp.zeros((row_count, 1), F32)
            for k in range(top):
                factor = factor + jnp.where(
                    cols[:, k : k + 1] == base + float(x), cols[:, top + k : top + k + 1], 0.0
                )
            term = terms[x] * factor
            total = term if total is None else total + term
        return total

    def back_step(d):
        if not isinstance(d, int):
            hidden_x(d).forward()
        back[z_at(d)] = routed_out(d).astype(BF)
        back_to(d).start()

    each(1, n_z, back_step)
    result = routed_out(0)

    loads[13].wait()
    shared_x.finish()
    for k in range(n_tp):
        result = result + dot(shared[k], common_d[pl.ds(k * hid, hid)])

    for d in range(1, n_tp):
        part_to(d).wait_recv()
    summed = part[t].astype(F32)
    for d in range(1, n_tp):
        summed = summed + part_in[d].astype(F32)
    token_out[...] = summed.astype(BF)

    for d in range(1, n_z):
        back_to(d).wait_recv()
    for d in range(1, n_z):
        result = result + back_in[d].astype(F32)
    expert_out[...] = result.astype(BF)

    swap_up.wait_send()
    swap_down.wait_send()
    for d in range(1, n_z):
        rows_z(d).wait_send()
        meta_z(d).wait_send()
        map_z(d).wait_send()
        back_to(d).wait_send()
        rows_x(d).sent()
    for d in range(n_z):
        map_on(d, c).wait_send()
        hidden_x(d).sent()
    shared_x.sent()
    for k in range(1, n_tp):
        part_to(k).wait_send()


def on_device(n_ep, n_tp, *args):
    (
        receptance, key_tensor, value_tensor, decay_data_input, correction_rate_input,
        mixer_output_gate, decay_channel_offset, head_norm_gain, self_key_weight,
        mixer_output_weight, second_batch_rows, routed_expert_index, routing_output_weight,
        expert_norm_gain, expert_gate_weight, expert_up_weight, expert_down_weight,
        common_expert_gate, common_expert_up, common_expert_down,
    ) = args
    n_z = n_ep // 2
    positions, width = receptance.shape
    row_count, model = second_batch_rows.shape
    top = routed_expert_index.shape[1]
    cap = 3 * row_count * top // (2 * n_ep)
    cap = -(-cap // 16) * 16
    hid = common_expert_gate.shape[0]
    units = common_expert_down.shape[0]
    piece = model // n_tp
    group = min(256, width)
    spans = positions // SPAN
    any_spec = pl.BlockSpec(memory_space=pl.ANY)
    vmem = pl.BlockSpec(memory_space=pltpu.VMEM)
    dma = pltpu.SemaphoreType.DMA
    share = positions // n_tp
    found = pl.pallas_call(
        functools.partial(whole_kernel, (n_z, n_tp, top, cap)),
        out_shape=(
            jax.ShapeDtypeStruct((share, model), BF),
            jax.ShapeDtypeStruct((row_count, piece), BF),
        ),
        in_specs=[any_spec] * 6 + [vmem] * 3 + [any_spec] + [any_spec, vmem, vmem, vmem] + [any_spec] * 6,
        out_specs=(vmem, vmem),
        scratch_shapes=[
            pltpu.VMEM((5, positions, width), BF),
            pltpu.VMEM((positions, width), BF),
            pltpu.VMEM((width, model), BF),
            pltpu.VMEM((row_count, model), BF),
            pltpu.VMEM((n_tp, n_z, row_count, piece), BF),
            pltpu.VMEM((n_z, 2 * top, row_count), F32),
            pltpu.VMEM((2, 2 * hid, model), BF),
            pltpu.VMEM((2, units, piece), BF),
            pltpu.VMEM((2 * hid, model), BF),
            pltpu.VMEM((units, piece), BF),
            pltpu.VMEM((n_z, 2, row_count, cap), BF),
            pltpu.VMEM((n_tp, n_z, 2 * cap, hid), BF),
            pltpu.VMEM((n_tp, row_count, hid), BF),
            pltpu.VMEM((n_tp, share, model), BF),
            pltpu.VMEM((n_tp, share, model), BF),
            pltpu.VMEM((n_z, row_count, piece), BF),
            pltpu.VMEM((n_z, row_count, piece), BF),
            pltpu.VMEM((n_z, 2, HEAD, 2 * width), BF),
            pltpu.VMEM((2, positions, width), F32),
            pltpu.VMEM((2, spans, HEAD, width), F32),
            pltpu.VMEM((positions, width), BF),
            pltpu.VMEM((group, group), BF),
            dma((14,)),
            dma((n_z,)), dma((n_z,)), dma((n_z,)), dma((n_z,)),
            dma((n_z, n_tp)), dma((n_z, n_tp)), dma((n_z, n_tp)), dma((n_z, n_tp)),
            dma((n_tp,)), dma((n_tp,)),
            dma((n_z,)), dma((n_z,)), dma((n_z,)), dma((n_z,)),
            dma((n_tp,)), dma((n_tp,)),
            dma((n_z,)), dma((n_z,)),
            dma((2,)), dma((2,)),
        ],
        compiler_params=pltpu.CompilerParams(
            collective_id=0, has_side_effects=True, vmem_limit_bytes=60 * 1024 * 1024
        ),
        name="mixer_and_experts",
    )(
        receptance, key_tensor, value_tensor, decay_data_input, correction_rate_input,
        mixer_output_gate, decay_channel_offset[None], head_norm_gain[None],
        self_key_weight[None], mixer_output_weight, second_batch_rows,
        routed_expert_index.T, routing_output_weight.T,
        expert_norm_gain[None], expert_gate_weight, expert_up_weight, expert_down_weight,
        common_expert_gate, common_expert_up, common_expert_down,
    )
    return pl.pallas_call(
        put_kernel,
        out_shape=tuple(jax.ShapeDtypeStruct(x.shape, x.dtype) for x in found),
        in_specs=[vmem] * 2,
        out_specs=(any_spec, any_spec),
        scratch_shapes=[dma((2,))],
        name="put_results",
    )(*found)


def put_kernel(token_in, expert_in, token_out, expert_out, sems):
    copies = [
        pltpu.make_async_copy(token_in, token_out, sems.at[0]),
        pltpu.make_async_copy(expert_in, expert_out, sems.at[1]),
    ]
    for copy in copies:
        copy.start()
    for copy in copies:
        copy.wait()


def solution(mesh):
    in_specs = (
        (P("ep", "tp"),) * 6
        + (P("tp"),) * 3
        + (P("tp", None),)
        + (P("ep", None),) * 3
        + (P(), P("ep", "tp", None), P("ep", "tp", None), P("ep", None, "tp"))
        + (P("tp", None), P("tp", None), P(None, "tp"))
    )
    out_specs = (P(("ep", "tp"), None), P("ep", "tp"))
    return jax.shard_map(
        functools.partial(on_device, mesh.shape["ep"], mesh.shape["tp"]),
        mesh=mesh, in_specs=in_specs, out_specs=out_specs, check_vma=False,
    )
```

```python
import functools
import math

import jax
import jax.numpy as jnp
from jax import lax
from jax.experimental import pallas as pl
from jax.experimental.pallas import tpu as pltpu
from jax.sharding import PartitionSpec as P

HEAD = 64
SPAN = 64
SPANS_AT_ONCE = 2
STRAIGHT = (("rows", 3), ("hidden", 3))
NORM_FLOOR = 1.0
F32 = jnp.float32
BF = jnp.bfloat16
MESH = pl.DeviceIdType.MESH
DIMS = {
    "nn": (((1,), (0,)), ((), ())),
    "nt": (((1,), (1,)), ((), ())),
    "tn": (((0,), (0,)), ((), ())),
}


def dot(a, b, form="nn"):
    return lax.dot_general(a, b, DIMS[form], preferred_element_type=F32)


def split(x):
    high = x.astype(BF)
    return high, (x - high.astype(F32)).astype(BF)


def spread(x, mask):
    lanes = min(128, x.shape[1])
    tiles = x.shape[1] // lanes
    none = jnp.zeros((lanes, lanes), x.dtype)
    columns = []
    for j in range(tiles):
        piece = x[:, j * lanes : (j + 1) * lanes]
        block = jnp.concatenate([piece] * (lanes // HEAD), axis=0) * mask
        columns.append(jnp.concatenate([none] * j + [block] + [none] * (tiles - 1 - j), axis=0))
    return columns[0] if tiles == 1 else jnp.concatenate(columns, axis=1)


def per_head(a, b, mask, form="nn", fine=False):
    return per_heads([a], [b], mask, form, fine)[0]


def per_heads(lefts, rights, mask, form="nn", fine=False):
    if not fine:
        return [
            dot(a.astype(BF), spread(b.astype(BF), mask), form) for a, b in zip(lefts, rights)
        ]
    lefts, rights = [split(a) for a in lefts], [split(b) for b in rights]
    both = [
        dot(jnp.concatenate(a, axis=0), spread(b[0], mask), form) for a, b in zip(lefts, rights)
    ]
    rest = [dot(a[0], spread(b[1], mask), form) for a, b in zip(lefts, rights)]
    rows = lefts[0][0].shape[0]
    return [x[:rows] + x[rows:] + y for x, y in zip(both, rest)]


def head_sums(xs, ones):
    rows = xs[0].shape[0]
    both = [dot(jnp.concatenate(split(x), axis=0), ones) for x in xs]
    return [x[:rows] + x[rows:] for x in both]


def fold(full):
    lanes = min(128, full.shape[1])
    low = lax.broadcasted_iota(jnp.int32, (HEAD, lanes), 1) < HEAD
    out = []
    for j in range(full.shape[1] // lanes):
        block = full[:, j * lanes : (j + 1) * lanes]
        at = j * lanes
        out.append(
            jnp.where(low, block[at : at + HEAD], block[at + HEAD : at + 2 * HEAD])
            if lanes > HEAD
            else block[at : at + HEAD]
        )
    return out[0] if len(out) == 1 else jnp.concatenate(out, axis=1)


def iotas(rows, lanes):
    at = lax.broadcasted_iota(jnp.int32, (rows, lanes), 0)
    s = lax.broadcasted_iota(jnp.int32, (rows, lanes), 1) & (HEAD - 1)
    return at, s


def local_spans(problems, mask, ones):
    group = problems[0][0].shape[1]
    at, s = iotas(SPAN, group)
    zero = jnp.zeros((SPAN, group), F32)
    row = lax.broadcasted_iota(jnp.int32, (SPAN, SPAN), 0)
    col = lax.broadcasted_iota(jnp.int32, (SPAN, SPAN), 1)
    reach = jnp.where(row >= col, 1.0, 0.0).astype(BF)
    many = range(len(problems))
    recepts = [p[0].astype(F32) for p in problems]
    keys = [p[1].astype(F32) for p in problems]
    values = [p[2] for p in problems]
    step = [-math.exp(-0.5) * jax.nn.sigmoid(p[5] + p[3].astype(F32)) for p in problems]
    parts = [split(x) for x in step]
    high = [dot(reach, x[0]) for x in parts]
    low = [dot(reach, x[1]) for x in parts]
    total = [x + y for x, y in zip(high, low)]
    squares = head_sums([k * k for k in keys], ones)
    units = [k * lax.rsqrt(q + 1.0) for k, q in zip(keys, squares)]
    fixes = [u * jax.nn.sigmoid(p[4].astype(F32)) for u, p in zip(units, problems)]
    grown = [jnp.exp(-x) for x in total]
    unit_in = [units[i] * jnp.exp(total[i] - step[i]) for i in many]
    recept_in = [recepts[i] * jnp.exp(total[i]) for i in many]
    left = [jnp.concatenate([unit_in[i], recept_in[i]], axis=0) for i in many]
    fix_scores = per_heads(left, [fixes[i] * grown[i] for i in many], mask, "nt")
    key_scores = per_heads(left, [keys[i] * grown[i] for i in many], mask, "nt")
    unit_fix = [jnp.where(at > s, x[:SPAN], zero) for x in fix_scores]
    read_fix = [jnp.where(at >= s, x[SPAN:], zero) for x in fix_scores]
    both_key = [
        jnp.concatenate(
            [jnp.where(at > s, x[:SPAN], zero), jnp.where(at >= s, x[SPAN:], zero)], axis=0
        )
        for x in key_scores
    ]
    key_values = per_heads(both_key, values, mask)
    inverse = None
    for level in range(SPAN.bit_length() - 1):
        pair = (
            ((at >> (level + 1)) == (s >> (level + 1)))
            & (((at >> level) & 1) == 1)
            & (((s >> level) & 1) == 0)
        )
        below = [jnp.where(pair, x, zero) for x in unit_fix]
        if inverse is None:
            inverse = [jnp.where(at == s, 1.0, 0.0) - x for x in below]
        else:
            first = per_heads(inverse, below, mask)
            second = per_heads(first, inverse, mask)
            inverse = [x - y for x, y in zip(inverse, second)]
    solved_state = per_heads(inverse, unit_in, mask)
    solved_value = per_heads(inverse, [x[:SPAN] for x in key_values], mask)
    from_state = per_heads(read_fix, solved_state, mask)
    from_value = per_heads(read_fix, solved_value, mask)
    last = [x[SPAN - 1 : SPAN] for x in total]
    tail = [jnp.exp(last[i] - total[i]) for i in many]
    fix_tail = [(-fixes[i] * tail[i]).astype(BF) for i in many]
    key_tail = [(keys[i] * tail[i]).astype(BF) for i in many]
    moves = [dot(fix_tail[i], solved_state[i].astype(BF), "tn") for i in many]
    adds = [
        dot(
            jnp.concatenate([key_tail[i], fix_tail[i]], axis=0),
            jnp.concatenate([values[i], solved_value[i].astype(BF)], axis=0),
            "tn",
        )
        for i in many
    ]
    return [
        (
            recept_in[i] - from_state[i],
            key_values[i][SPAN:] - from_value[i],
            fold(moves[i]) + jnp.where(at == s, jnp.exp(last[i]), zero),
            fold(adds[i]),
        )
        for i in many
    ]


def silu(v):
    return v / (1.0 + jnp.exp(-v))


def whole_kernel(
    sizes,
    recept_in, keys_in, values_in, data_in, rate_in, gate_in,
    offset_in, gain_in, self_in, out_weight_in,
    second_in, ids_in, factor_in, norm_in,
    gate_w_in, up_w_in, down_w_in, common_gate_in, common_up_in, common_down_in,
    token_out, expert_out,
    mix, gate_v, out_w, second, rows, meta, gate_up, down, common, common_d,
    picks, hidden, shared, part, part_in, back, back_in, pair, chip, reads, steps, mixed, mask_v,
    load_s, zs, zr, ms, mr, rs, rr, hs, hr, cs, cr, ps, pr, fs, fr, os, orr, bs, br, ws, wr,
):
    n_z, n_tp, top, cap = sizes
    e = lax.axis_index("ep")
    t = lax.axis_index("tp")
    z = e // 2
    c = e % 2
    positions, width = recept_in.shape
    group = min(256, width)
    groups = width // group
    lane_tile = min(128, group)
    spans = positions // SPAN
    row_count, model = second_in.shape
    piece = model // n_tp
    hid = common_gate_in.shape[0]

    partner = (e + 1 - 2 * c, t)

    line = n_z == 4

    def z_to(d):
        if line:
            return (z, z + 1 - 2 * (z % 2), (z + 2) % 4, 3 - z)[d]
        return (z + d) % n_z

    def z_at(d):
        if line:
            return z_to(d)
        return (z - d + n_z) % n_z

    def z_dev(d):
        return (z_to(d) * 2 + c, t)

    def back_dev(d):
        return (z_at(d) * 2 + c, t)

    def tp_dev(d):
        return (e, (t + d) % n_tp)

    def send(src, dst, ssem, rsem, dev):
        return pltpu.make_async_remote_copy(
            src_ref=src, dst_ref=dst, send_sem=ssem, recv_sem=rsem,
            device_id=dev, device_id_type=MESH,
        )

    def load(src, dst, k):
        return pltpu.make_async_copy(src, dst, load_s.at[k])

    loads = [
        load(second_in, second, 0),
        load(common_gate_in, common.at[pl.ds(0, hid)], 1),
        load(common_up_in, common.at[pl.ds(hid, hid)], 2),
        load(gate_w_in.at[0], gate_up.at[c, pl.ds(0, hid)], 3),
        load(up_w_in.at[0], gate_up.at[c, pl.ds(hid, hid)], 4),
        load(recept_in, mix.at[0], 5),
        load(keys_in, mix.at[1], 6),
        load(values_in, mix.at[2], 7),
        load(data_in, mix.at[3], 8),
        load(rate_in, mix.at[4], 9),
        load(gate_in, gate_v, 10),
        load(down_w_in.at[0], down.at[c], 11),
        load(out_weight_in, out_w, 12),
        load(common_down_in, common_d, 13),
    ]
    loads[0].start()

    barrier = pltpu.get_barrier_semaphore()
    peers = [partner] + [z_dev(d) for d in range(1, n_z)] + [tp_dev(d) for d in range(1, n_tp)]
    for dev in peers:
        pl.semaphore_signal(barrier, inc=1, device_id=dev, device_id_type=MESH)
    for copy in loads[1:5]:
        copy.start()

    r_i = lax.broadcasted_iota(jnp.int32, (group, group), 0)
    c_i = lax.broadcasted_iota(jnp.int32, (group, group), 1)
    mask_v[...] = jnp.where((r_i >> 6) == (c_i >> 6), 1.0, 0.0).astype(BF)
    meta[z] = jnp.concatenate([ids_in[...].astype(F32), factor_in[...]], axis=0)
    loads[0].wait()
    wide = second[...].astype(F32)
    scale = lax.rsqrt(jnp.mean(wide * wide, axis=-1, keepdims=True) + NORM_FLOOR)
    for k in range(n_tp):
        lanes = pl.ds(k * piece, piece)
        rows[k, z] = (
            second[:, lanes].astype(F32) * scale * norm_in[:, lanes]
        ).astype(BF)
    for copy in loads[5:]:
        copy.start()

    pl.semaphore_wait(barrier, len(peers))

    def rows_z(d):
        return send(rows.at[t, z], rows.at[t, z], zs.at[d], zr.at[d], z_dev(d))

    def rows_z_wait(d):
        w = z_at(d)
        return send(rows.at[t, w], rows.at[t, w], zs.at[d], zr.at[d], z_dev(d))

    def meta_z(d):
        return send(meta.at[z], meta.at[z], ms.at[d], mr.at[d], z_dev(d))

    def meta_z_wait(d):
        w = z_at(d)
        return send(meta.at[w], meta.at[w], ms.at[d], mr.at[d], z_dev(d))

    for d in range(1, n_z):
        rows_z(d).start()
    for d in range(1, n_z):
        meta_z(d).start()
    for copy in loads[3:5]:
        copy.wait()
    swap_up = send(gate_up.at[c], gate_up.at[c], ws.at[0], wr.at[0], partner)
    swap_up_in = send(gate_up.at[1 - c], gate_up.at[1 - c], ws.at[0], wr.at[0], partner)
    swap_down = send(down.at[c], down.at[c], ws.at[1], wr.at[1], partner)
    swap_down_in = send(down.at[1 - c], down.at[1 - c], ws.at[1], wr.at[1], partner)
    swap_up.start()

    square = n_tp == 4
    if square:
        x_t, y_t, far_t = t + 1 - 2 * (t % 2), (t + 2) % 4, 3 - t
        x_dev, y_dev = (e, x_t), (e, y_t)

    class Exchange:
        def __init__(self, whole, half, sem_s, sem_r, straight):
            self.whole, self.half, self.sem_s, self.sem_r = whole, half, sem_s, sem_r
            self.relayed = square and not straight

        def copy(self, ref, k, dev):
            return send(ref, ref, self.sem_s(k), self.sem_r(k), dev)

        def first(self):
            if square:
                near = [self.copy(self.whole(t), 1, x_dev), self.copy(self.whole(t), 2, y_dev)]
                far = [self.copy(self.whole(t), 3, (e, far_t))]
                return near + ([] if self.relayed else far)
            return [self.copy(self.whole(t), k, tp_dev(k)) for k in range(1, n_tp)]

        def second(self):
            if self.relayed:
                return [
                    self.copy(self.half(x_t, 0), 3, y_dev),
                    self.copy(self.half(y_t, 1), 0, x_dev),
                ]
            return []

        def start(self):
            for copy in self.first():
                copy.start()

        def near_in(self):
            return [self.copy(self.whole(x_t), 1, x_dev), self.copy(self.whole(y_t), 2, y_dev)]

        def forward(self):
            if self.relayed:
                for came, copy in zip(self.near_in(), self.second()):
                    came.wait_recv()
                    copy.start()

        def finish(self):
            if self.relayed:
                self.copy(self.half(far_t, 0), 3, y_dev).wait_recv()
                self.copy(self.half(far_t, 1), 0, x_dev).wait_recv()
            elif square:
                for came in self.near_in() + [self.copy(self.whole(far_t), 3, (e, far_t))]:
                    came.wait_recv()
            else:
                for k in range(1, n_tp):
                    src = (t - k + n_tp) % n_tp
                    self.copy(self.whole(src), k, tp_dev(k)).wait_recv()

        def sent(self):
            for copy in self.first() + self.second():
                copy.wait_send()

    def straight(kind, d):
        return line and (kind, d) in STRAIGHT

    half_rows = row_count // 2
    shared_x = Exchange(
        lambda src: shared.at[src],
        lambda src, i: shared.at[src, pl.ds(i * half_rows, half_rows)],
        lambda k: cs.at[k], lambda k: cr.at[k], False,
    )

    def rows_x(d):
        zz = z_at(d)
        return Exchange(
            lambda src: rows.at[src, zz],
            lambda src, i: rows.at[src, zz, pl.ds(i * half_rows, half_rows)],
            lambda k: rs.at[d, k], lambda k: rr.at[d, k], straight("rows", d),
        )

    def hidden_x(d):
        zz = z_at(d)
        return Exchange(
            lambda src: hidden.at[src, zz],
            lambda src, i: hidden.at[src, zz, pl.ds(i * cap, cap)],
            lambda k: hs.at[d, k], lambda k: hr.at[d, k], straight("hidden", d),
        )

    def each(low, high, step):
        if high - low <= 4:
            for d in range(low, high):
                step(d)
        else:
            def body(d, carry):
                step(d)
                return carry

            lax.fori_loop(low, high, body, 0)

    def both_dots(zz, weights):
        totals = [None] * len(weights)
        for i, weight in enumerate(weights):
            for k in range(n_tp):
                term = dot(rows[k, zz], weight[:, k * piece : (k + 1) * piece], "nt")
                totals[i] = term if totals[i] is None else totals[i] + term
        return [(silu(total[:, :hid]) * total[:, hid:]).astype(BF) for total in totals]

    for copy in loads[1:3]:
        copy.wait()
    shared[t] = both_dots(z, [common])[0]
    shared_x.start()

    def routes(zz):
        cols = jnp.transpose(meta[zz])
        base = (z * 2).astype(F32)
        return cols, base

    def routed(d):
        zz = z_at(d)
        cols, base = routes(zz)
        lane = lax.broadcasted_iota(jnp.int32, (row_count, 128), 1).astype(F32) + base
        named = jnp.zeros((row_count, 128), F32)
        for k in range(top):
            named = named + jnp.where(cols[:, k : k + 1] == lane, 1.0, 0.0)
        row = lax.broadcasted_iota(jnp.int32, (row_count, row_count), 0)
        col = lax.broadcasted_iota(jnp.int32, (row_count, row_count), 1)
        rank = dot(jnp.where(row > col, 1.0, 0.0).astype(BF), named.astype(BF))
        slot = lax.broadcasted_iota(jnp.int32, (row_count, cap), 1).astype(F32)
        units = both_dots(zz, [gate_up[0], gate_up[1]])
        chosen = [
            jnp.where(
                slot == rank[:, x : x + 1],
                jnp.broadcast_to(named[:, x : x + 1], (row_count, cap)),
                0.0,
            ).astype(BF)
            for x in range(2)
        ]
        packed = [dot(chosen[x], units[x], "tn").astype(BF) for x in range(2)]
        for x in range(2):
            picks[zz, x] = chosen[x]
            hidden[t, zz, pl.ds(x * cap, cap)] = packed[x]
        hidden_x(d).start()

    def relay(d):
        rows_z_wait(d).wait_recv()
        rows_x(d).start()

    stride = SPANS_AT_ONCE if spans % SPANS_AT_ONCE == 0 else 1

    def span_step(i):
        where = [
            (i * stride + j, pl.ds((i * stride + j) * SPAN, SPAN), pl.ds(g * group, group))
            for j in range(stride)
            for g in range(groups)
        ]
        found = local_spans(
            [
                tuple(mix[k, span, lanes] for k in range(5)) + (offset_in[:, lanes],)
                for _, span, lanes in where
            ],
            mask_v[:lane_tile, :lane_tile],
            mask_v[...],
        )
        for (b, span, lanes), (read_state, read_value, move, add) in zip(where, found):
            reads[0, span, lanes] = read_state
            reads[1, span, lanes] = read_value
            steps[0, b, :, lanes] = move
            steps[1, b, :, lanes] = add

    tiles = [pl.ds(g * group, group) for g in range(groups)]
    wide = width // 2

    def small_mask():
        return mask_v[: min(128, wide), : min(128, wide)]

    def compose_own():
        mask = mask_v[:lane_tile, :lane_tile]
        now = [steps[k, 0, :, lanes] for k in range(2) for lanes in tiles]
        for b in range(1, spans):
            now = per_heads([steps[0, b, :, lanes] for lanes in tiles] * 2, now, mask, fine=True)
            for g, lanes in enumerate(tiles):
                now[groups + g] = now[groups + g] + steps[1, b, :, lanes]
        for k in range(2):
            both = now[k * groups : (k + 1) * groups]
            both = both[0] if groups == 1 else jnp.concatenate(both, axis=1)
            for h in range(2):
                pair[c, h, :, k * wide : (k + 1) * wide] = both[
                    :, h * wide : (h + 1) * wide
                ].astype(BF)

    def pair_on(core):
        return send(pair.at[core], pair.at[core], ps.at[0], pr.at[0], partner)

    def chip_z(d, zz):
        return send(chip.at[zz, c], chip.at[zz, c], ps.at[d], pr.at[d], z_dev(d))

    def chip_on(d, half):
        zz = z_at(d)
        return send(chip.at[zz, half], chip.at[zz, half], fs.at[d], fr.at[d], partner)

    def apply(before, now, mask):
        new = per_heads([now[:, :wide].astype(F32)] * len(before), before, mask, fine=True)
        new[-1] = new[-1] + now[:, wide:].astype(F32)
        return new

    def compose_chip():
        pair_on(1 - c).wait_recv()
        first = pair[0, c].astype(F32)
        new = apply([first[:, :wide], first[:, wide:]], pair[1, c], small_mask())
        for k in range(2):
            chip[z, c, :, k * wide : (k + 1) * wide] = new[k].astype(BF)
        for d in range(1, n_z):
            chip_z(d, z).start()

    def chips_forward():
        for d in range(1, n_z):
            chip_z(d, z_at(d)).wait_recv()
            chip_on(d, c).start()

    def finish_mixer():
        for d in range(1, n_z):
            chip_on(d, 1 - c).wait_recv()

        def prefix(i, state):
            return [apply([state[h]], chip[i, h], small_mask())[0] for h in range(2)]

        state = lax.fori_loop(0, z, prefix, [jnp.zeros((HEAD, wide), F32) for _ in range(2)])
        behind = [apply([state[h]], pair[0, h], small_mask())[0] for h in range(2)]
        state = [jnp.where(c == 1, behind[h], state[h]) for h in range(2)]
        if wide != group:
            state = jnp.concatenate(state, axis=1)
            state = [state[:, g * group : (g + 1) * group] for g in range(groups)]
        loads[10].wait()

        def finish_step(b, state):
            span = pl.ds(b * SPAN, SPAN)
            mask, ones = mask_v[:lane_tile, :lane_tile], mask_v[...]
            many = range(groups)
            recepts = [mix[0, span, lanes].astype(F32) for lanes in tiles]
            keys = [mix[1, span, lanes].astype(F32) for lanes in tiles]
            own = [recepts[g] * keys[g] * self_in[:, tiles[g]] for g in many]
            both = per_heads(
                [
                    jnp.concatenate([reads[0, span, lanes], steps[0, b, :, lanes]], axis=0)
                    for lanes in tiles
                ],
                state, mask, fine=True,
            )
            following = [both[g][SPAN:] + steps[1, b, :, tiles[g]] for g in many]
            read = [reads[1, span, tiles[g]] + both[g][:SPAN] for g in many]
            sums = head_sums([jnp.concatenate([read[g], own[g]], axis=0) for g in many], ones)
            apart = [read[g] - sums[g][:SPAN] * (1.0 / HEAD) for g in many]
            squares = head_sums([x * x for x in apart], ones)
            for g, lanes in enumerate(tiles):
                normed = (
                    apart[g]
                    * lax.rsqrt(squares[g] * (1.0 / HEAD) + NORM_FLOOR)
                    * gain_in[:, lanes]
                )
                out = (normed + sums[g][SPAN:] * mix[2, span, lanes].astype(F32)) * gate_v[
                    span, lanes
                ].astype(F32)
                mixed[span, lanes] = out.astype(BF)
            return following

        for b in range(spans):
            state = finish_step(b, state)

    share = positions // n_tp
    wide_cols = min(512, model)

    def project():
        loads[12].wait()
        for i in range(model // wide_cols):
            lanes = pl.ds(i * wide_cols, wide_cols)
            got = dot(mixed[...], out_w[:, lanes]).astype(BF)
            for k in range(n_tp):
                part[k, :, lanes] = got[k * share : (k + 1) * share]

    def part_to(d):
        return send(
            part.at[(t + d) % n_tp], part_in.at[d], os.at[d], orr.at[d], tp_dev(d)
        )

    half_model = model // 2

    def cut(h):
        return pl.ds(h * half_model, half_model)

    def pair_to(h, j):
        k = (x_t + 2 * j) % 4 if h == 0 else (y_t + j * (1 - 2 * (t % 2))) % 4
        dev = x_dev if h == 0 else y_dev
        i = 2 * h + j
        return send(part.at[k, :, cut(h)], part_in.at[j, :, cut(h)], os.at[i], orr.at[i], dev)

    def sum_to(h):
        dev = y_dev if h == 0 else x_dev
        return send(
            part_in.at[2, :, cut(h)], part_in.at[3, :, cut(h)], os.at[4 + h], orr.at[4 + h], dev
        )

    def parts_start():
        if square:
            for h in range(2):
                for j in (1, 0):
                    pair_to(h, j).start()
        else:
            for d in range(1, n_tp):
                part_to(d).start()

    def parts_turn():
        for h in range(2):
            k = y_t if h == 0 else x_t
            pair_to(h, 1).wait_recv()
            part_in[2, :, cut(h)] = (
                part[k, :, cut(h)].astype(F32) + part_in[1, :, cut(h)].astype(F32)
            ).astype(BF)
            sum_to(h).start()

    def parts_sum():
        if square:
            out = []
            for h in range(2):
                pair_to(h, 0).wait_recv()
                sum_to(h).wait_recv()
                out.append(
                    part[t, :, cut(h)].astype(F32)
                    + part_in[0, :, cut(h)].astype(F32)
                    + part_in[3, :, cut(h)].astype(F32)
                )
            return jnp.concatenate(out, axis=1)
        summed = part[t].astype(F32)
        for d in range(1, n_tp):
            part_to(d).wait_recv()
            summed = summed + part_in[d].astype(F32)
        return summed

    def back_to(d):
        return send(back.at[z_at(d)], back_in.at[d], bs.at[d], br.at[d], back_dev(d))

    def routed_out(d):
        zz = z_at(d)
        cols, base = routes(zz)
        hidden_x(d).finish()
        copies = [None, None]
        for x in range(2):
            for k in range(n_tp):
                term = dot(
                    hidden[k, zz, pl.ds(x * cap, cap)], down[x, pl.ds(k * hid, hid)]
                )
                copies[x] = term if copies[x] is None else copies[x] + term
        terms = [dot(picks[zz, x], copies[x].astype(BF)) for x in range(2)]
        total = None
        for x in range(2):
            factor = jnp.zeros((row_count, 1), F32)
            for k in range(top):
                factor = factor + jnp.where(
                    cols[:, k : k + 1] == base + float(x), cols[:, top + k : top + k + 1], 0.0
                )
            term = terms[x] * factor
            total = term if total is None else total + term
        return total

    def send_back(d):
        back[z_at(d)] = routed_out(d).astype(BF)
        back_to(d).start()

    def other(d):
        meta_z_wait(d).wait_recv()
        rows_x(d).finish()
        routed(d)

    for copy in loads[5:10]:
        copy.wait()
    span_step(0)
    if line:
        relay(1)
    swap_up_in.wait_recv()
    routed(0)
    shared_x.forward()
    loads[11].wait()
    swap_down.start()
    for i in range(1, spans // stride):
        span_step(i)
    if line:
        rows_x(1).forward()
    compose_own()
    pair_on(c).start()
    if line:
        relay(2)
    hidden_x(0).forward()
    if line:
        compose_chip()
        other(1)
        rows_x(2).forward()
        relay(3)
        other(2)
        hidden_x(1).forward()
        chips_forward()
        rows_x(3).forward()
        hidden_x(2).forward()
        other(3)
        hidden_x(3).forward()
        swap_down_in.wait_recv()
        send_back(1)
        send_back(2)
        finish_mixer()
        project()
        parts_start()
        send_back(3)
        if square:
            parts_turn()
    else:
        compose_chip()
        each(1, n_z, relay)
        each(1, n_z, lambda d: rows_x(d).forward())
        each(1, n_z, other)
        each(1, n_z, lambda d: hidden_x(d).forward())
        swap_down_in.wait_recv()
        each(1, n_z, send_back)
        chips_forward()
        finish_mixer()
        project()
        parts_start()
    result = routed_out(0)
    loads[13].wait()
    shared_x.finish()
    for k in range(n_tp):
        result = result + dot(shared[k], common_d[pl.ds(k * hid, hid)])

    if square and not line:
        parts_turn()
    summed = parts_sum()
    token_out[...] = summed.astype(BF)

    for d in range(1, n_z):
        back_to(d).wait_recv()
    for d in range(1, n_z):
        result = result + back_in[d].astype(F32)
    expert_out[...] = result.astype(BF)

    swap_up.wait_send()
    swap_down.wait_send()
    for d in range(1, n_z):
        rows_z(d).wait_send()
        meta_z(d).wait_send()
        chip_z(d, z).wait_send()
        chip_on(d, c).wait_send()
        back_to(d).wait_send()
        rows_x(d).sent()
    pair_on(c).wait_send()
    for d in range(n_z):
        hidden_x(d).sent()
    shared_x.sent()
    if square:
        for h in range(2):
            sum_to(h).wait_send()
            for j in range(2):
                pair_to(h, j).wait_send()
    else:
        for k in range(1, n_tp):
            part_to(k).wait_send()


def on_device(n_ep, n_tp, *args):
    (
        receptance, key_tensor, value_tensor, decay_data_input, correction_rate_input,
        mixer_output_gate, decay_channel_offset, head_norm_gain, self_key_weight,
        mixer_output_weight, second_batch_rows, routed_expert_index, routing_output_weight,
        expert_norm_gain, expert_gate_weight, expert_up_weight, expert_down_weight,
        common_expert_gate, common_expert_up, common_expert_down,
    ) = args
    n_z = n_ep // 2
    positions, width = receptance.shape
    row_count, model = second_batch_rows.shape
    top = routed_expert_index.shape[1]
    cap = 3 * row_count * top // (2 * n_ep)
    cap = -(-cap // 16) * 16
    hid = common_expert_gate.shape[0]
    units = common_expert_down.shape[0]
    piece = model // n_tp
    group = min(256, width)
    spans = positions // SPAN
    any_spec = pl.BlockSpec(memory_space=pl.ANY)
    vmem = pl.BlockSpec(memory_space=pltpu.VMEM)
    dma = pltpu.SemaphoreType.DMA
    share = positions // n_tp
    found = pl.pallas_call(
        functools.partial(whole_kernel, (n_z, n_tp, top, cap)),
        out_shape=(
            jax.ShapeDtypeStruct((share, model), BF),
            jax.ShapeDtypeStruct((row_count, piece), BF),
        ),
        in_specs=[any_spec] * 6 + [vmem] * 3 + [any_spec] + [any_spec, vmem, vmem, vmem] + [any_spec] * 6,
        out_specs=(vmem, vmem),
        scratch_shapes=[
            pltpu.VMEM((5, positions, width), BF),
            pltpu.VMEM((positions, width), BF),
            pltpu.VMEM((width, model), BF),
            pltpu.VMEM((row_count, model), BF),
            pltpu.VMEM((n_tp, n_z, row_count, piece), BF),
            pltpu.VMEM((n_z, 2 * top, row_count), F32),
            pltpu.VMEM((2, 2 * hid, model), BF),
            pltpu.VMEM((2, units, piece), BF),
            pltpu.VMEM((2 * hid, model), BF),
            pltpu.VMEM((units, piece), BF),
            pltpu.VMEM((n_z, 2, row_count, cap), BF),
            pltpu.VMEM((n_tp, n_z, 2 * cap, hid), BF),
            pltpu.VMEM((n_tp, row_count, hid), BF),
            pltpu.VMEM((n_tp, share, model), BF),
            pltpu.VMEM((n_tp, share, model), BF),
            pltpu.VMEM((n_z, row_count, piece), BF),
            pltpu.VMEM((n_z, row_count, piece), BF),
            pltpu.VMEM((2, 2, HEAD, width), BF),
            pltpu.VMEM((n_z, 2, HEAD, width), BF),
            pltpu.VMEM((2, positions, width), F32),
            pltpu.VMEM((2, spans, HEAD, width), F32),
            pltpu.VMEM((positions, width), BF),
            pltpu.VMEM((group, group), BF),
            dma((14,)),
            dma((n_z,)), dma((n_z,)), dma((n_z,)), dma((n_z,)),
            dma((n_z, n_tp)), dma((n_z, n_tp)), dma((n_z, n_tp)), dma((n_z, n_tp)),
            dma((n_tp,)), dma((n_tp,)),
            dma((n_z,)), dma((n_z,)), dma((n_z,)), dma((n_z,)),
            dma((max(6, n_tp),)), dma((max(6, n_tp),)),
            dma((n_z,)), dma((n_z,)),
            dma((2,)), dma((2,)),
        ],
        compiler_params=pltpu.CompilerParams(
            collective_id=0, has_side_effects=True, vmem_limit_bytes=60 * 1024 * 1024
        ),
        name="mixer_and_experts",
    )(
        receptance, key_tensor, value_tensor, decay_data_input, correction_rate_input,
        mixer_output_gate, decay_channel_offset[None], head_norm_gain[None],
        self_key_weight[None], mixer_output_weight, second_batch_rows,
        routed_expert_index.T, routing_output_weight.T,
        expert_norm_gain[None], expert_gate_weight, expert_up_weight, expert_down_weight,
        common_expert_gate, common_expert_up, common_expert_down,
    )
    return pl.pallas_call(
        put_kernel,
        out_shape=tuple(jax.ShapeDtypeStruct(x.shape, x.dtype) for x in found),
        in_specs=[vmem] * 2,
        out_specs=(any_spec, any_spec),
        scratch_shapes=[dma((2,))],
        name="put_results",
    )(*found)


def put_kernel(token_in, expert_in, token_out, expert_out, sems):
    copies = [
        pltpu.make_async_copy(token_in, token_out, sems.at[0]),
        pltpu.make_async_copy(expert_in, expert_out, sems.at[1]),
    ]
    for copy in copies:
        copy.start()
    for copy in copies:
        copy.wait()


def solution(mesh):
    in_specs = (
        (P("ep", "tp"),) * 6
        + (P("tp"),) * 3
        + (P("tp", None),)
        + (P("ep", None),) * 3
        + (P(), P("ep", "tp", None), P("ep", "tp", None), P("ep", None, "tp"))
        + (P("tp", None), P("tp", None), P(None, "tp"))
    )
    out_specs = (P(("ep", "tp"), None), P("ep", "tp"))
    return jax.shard_map(
        functools.partial(on_device, mesh.shape["ep"], mesh.shape["tp"]),
        mesh=mesh, in_specs=in_specs, out_specs=out_specs, check_vma=False,
    )
```

```python
import functools
import math

import jax
import jax.numpy as jnp
from jax import lax
from jax.experimental import pallas as pl
from jax.experimental.pallas import tpu as pltpu
from jax.sharding import PartitionSpec as P

HEAD = 64
SPAN = 64
SPANS_AT_ONCE = 2
STRAIGHT = (("rows", 3), ("hidden", 3))
NORM_FLOOR = 1.0
F32 = jnp.float32
BF = jnp.bfloat16
MESH = pl.DeviceIdType.MESH
DIMS = {
    "nn": (((1,), (0,)), ((), ())),
    "nt": (((1,), (1,)), ((), ())),
    "tn": (((0,), (0,)), ((), ())),
}


def dot(a, b, form="nn"):
    return lax.dot_general(a, b, DIMS[form], preferred_element_type=F32)


def split(x):
    high = x.astype(BF)
    return high, (x - high.astype(F32)).astype(BF)


def spread(x, mask):
    lanes = min(128, x.shape[1])
    tiles = x.shape[1] // lanes
    none = jnp.zeros((lanes, lanes), x.dtype)
    columns = []
    for j in range(tiles):
        piece = x[:, j * lanes : (j + 1) * lanes]
        block = jnp.concatenate([piece] * (lanes // HEAD), axis=0) * mask
        columns.append(jnp.concatenate([none] * j + [block] + [none] * (tiles - 1 - j), axis=0))
    return columns[0] if tiles == 1 else jnp.concatenate(columns, axis=1)


def per_head(a, b, mask, form="nn", fine=False):
    return per_heads([a], [b], mask, form, fine)[0]


def per_heads(lefts, rights, mask, form="nn", fine=False):
    if not fine:
        return [
            dot(a.astype(BF), spread(b.astype(BF), mask), form) for a, b in zip(lefts, rights)
        ]
    lefts, rights = [split(a) for a in lefts], [split(b) for b in rights]
    both = [
        dot(jnp.concatenate(a, axis=0), spread(b[0], mask), form) for a, b in zip(lefts, rights)
    ]
    rest = [dot(a[0], spread(b[1], mask), form) for a, b in zip(lefts, rights)]
    rows = lefts[0][0].shape[0]
    return [x[:rows] + x[rows:] + y for x, y in zip(both, rest)]


def head_sums(xs, ones):
    rows = xs[0].shape[0]
    both = [dot(jnp.concatenate(split(x), axis=0), ones) for x in xs]
    return [x[:rows] + x[rows:] for x in both]


def fold(full):
    lanes = min(128, full.shape[1])
    low = lax.broadcasted_iota(jnp.int32, (HEAD, lanes), 1) < HEAD
    out = []
    for j in range(full.shape[1] // lanes):
        block = full[:, j * lanes : (j + 1) * lanes]
        at = j * lanes
        out.append(
            jnp.where(low, block[at : at + HEAD], block[at + HEAD : at + 2 * HEAD])
            if lanes > HEAD
            else block[at : at + HEAD]
        )
    return out[0] if len(out) == 1 else jnp.concatenate(out, axis=1)


def iotas(rows, lanes):
    at = lax.broadcasted_iota(jnp.int32, (rows, lanes), 0)
    s = lax.broadcasted_iota(jnp.int32, (rows, lanes), 1) & (HEAD - 1)
    return at, s


def local_spans(problems, mask, ones):
    group = problems[0][0].shape[1]
    at, s = iotas(SPAN, group)
    zero = jnp.zeros((SPAN, group), F32)
    row = lax.broadcasted_iota(jnp.int32, (SPAN, SPAN), 0)
    col = lax.broadcasted_iota(jnp.int32, (SPAN, SPAN), 1)
    reach = jnp.where(row >= col, 1.0, 0.0).astype(BF)
    many = range(len(problems))
    recepts = [p[0].astype(F32) for p in problems]
    keys = [p[1].astype(F32) for p in problems]
    values = [p[2] for p in problems]
    step = [-math.exp(-0.5) * jax.nn.sigmoid(p[5] + p[3].astype(F32)) for p in problems]
    parts = [split(x) for x in step]
    high = [dot(reach, x[0]) for x in parts]
    low = [dot(reach, x[1]) for x in parts]
    total = [x + y for x, y in zip(high, low)]
    squares = head_sums([k * k for k in keys], ones)
    units = [k * lax.rsqrt(q + 1.0) for k, q in zip(keys, squares)]
    fixes = [u * jax.nn.sigmoid(p[4].astype(F32)) for u, p in zip(units, problems)]
    grown = [jnp.exp(-x) for x in total]
    unit_in = [units[i] * jnp.exp(total[i] - step[i]) for i in many]
    recept_in = [recepts[i] * jnp.exp(total[i]) for i in many]
    left = [jnp.concatenate([unit_in[i], recept_in[i]], axis=0) for i in many]
    fix_scores = per_heads(left, [fixes[i] * grown[i] for i in many], mask, "nt")
    key_scores = per_heads(left, [keys[i] * grown[i] for i in many], mask, "nt")
    unit_fix = [jnp.where(at > s, x[:SPAN], zero) for x in fix_scores]
    read_fix = [jnp.where(at >= s, x[SPAN:], zero) for x in fix_scores]
    both_key = [
        jnp.concatenate(
            [jnp.where(at > s, x[:SPAN], zero), jnp.where(at >= s, x[SPAN:], zero)], axis=0
        )
        for x in key_scores
    ]
    key_values = per_heads(both_key, values, mask)
    inverse = None
    for level in range(SPAN.bit_length() - 1):
        pair = (
            ((at >> (level + 1)) == (s >> (level + 1)))
            & (((at >> level) & 1) == 1)
            & (((s >> level) & 1) == 0)
        )
        below = [jnp.where(pair, x, zero) for x in unit_fix]
        if inverse is None:
            inverse = [jnp.where(at == s, 1.0, 0.0) - x for x in below]
        else:
            first = per_heads(inverse, below, mask)
            second = per_heads(first, inverse, mask)
            inverse = [x - y for x, y in zip(inverse, second)]
    solved_state = per_heads(inverse, unit_in, mask)
    solved_value = per_heads(inverse, [x[:SPAN] for x in key_values], mask)
    from_state = per_heads(read_fix, solved_state, mask)
    from_value = per_heads(read_fix, solved_value, mask)
    last = [x[SPAN - 1 : SPAN] for x in total]
    tail = [jnp.exp(last[i] - total[i]) for i in many]
    fix_tail = [(-fixes[i] * tail[i]).astype(BF) for i in many]
    key_tail = [(keys[i] * tail[i]).astype(BF) for i in many]
    moves = [dot(fix_tail[i], solved_state[i].astype(BF), "tn") for i in many]
    adds = [
        dot(
            jnp.concatenate([key_tail[i], fix_tail[i]], axis=0),
            jnp.concatenate([values[i], solved_value[i].astype(BF)], axis=0),
            "tn",
        )
        for i in many
    ]
    return [
        (
            recept_in[i] - from_state[i],
            key_values[i][SPAN:] - from_value[i],
            fold(moves[i]) + jnp.where(at == s, jnp.exp(last[i]), zero),
            fold(adds[i]),
        )
        for i in many
    ]


def silu(v):
    return v / (1.0 + jnp.exp(-v))


def whole_kernel(
    sizes,
    recept_in, keys_in, values_in, data_in, rate_in, gate_in,
    offset_in, gain_in, self_in, out_weight_in,
    second_in, ids_in, factor_in, norm_in,
    gate_w_in, up_w_in, down_w_in, common_gate_in, common_up_in, common_down_in,
    token_out, expert_out,
    mix, gate_v, out_w, second, rows, meta, gate_up, down, common, common_d,
    picks, hidden, shared, part, part_in, back, back_in, pair, chip, reads, steps, mixed, mask_v,
    load_s, zs, zr, ms, mr, rs, rr, hs, hr, cs, cr, ps, pr, fs, fr, os, orr, bs, br, ws, wr,
):
    n_z, n_tp, top, cap = sizes
    e = lax.axis_index("ep")
    t = lax.axis_index("tp")
    z = e // 2
    c = e % 2
    positions, width = recept_in.shape
    group = min(256, width)
    groups = width // group
    lane_tile = min(128, group)
    spans = positions // SPAN
    row_count, model = second_in.shape
    piece = model // n_tp
    hid = common_gate_in.shape[0]

    partner = (e + 1 - 2 * c, t)

    line = n_z == 4

    def z_to(d):
        if line:
            return (z, z + 1 - 2 * (z % 2), (z + 2) % 4, 3 - z)[d]
        return (z + d) % n_z

    def z_at(d):
        if line:
            return z_to(d)
        return (z - d + n_z) % n_z

    def z_dev(d):
        return (z_to(d) * 2 + c, t)

    def back_dev(d):
        return (z_at(d) * 2 + c, t)

    def tp_dev(d):
        return (e, (t + d) % n_tp)

    def send(src, dst, ssem, rsem, dev):
        return pltpu.make_async_remote_copy(
            src_ref=src, dst_ref=dst, send_sem=ssem, recv_sem=rsem,
            device_id=dev, device_id_type=MESH,
        )

    def load(src, dst, k):
        return pltpu.make_async_copy(src, dst, load_s.at[k])

    loads = [
        load(second_in, second, 0),
        load(common_gate_in, common.at[pl.ds(0, hid)], 1),
        load(common_up_in, common.at[pl.ds(hid, hid)], 2),
        load(gate_w_in.at[0], gate_up.at[c, pl.ds(0, hid)], 3),
        load(up_w_in.at[0], gate_up.at[c, pl.ds(hid, hid)], 4),
        load(recept_in, mix.at[0], 5),
        load(keys_in, mix.at[1], 6),
        load(values_in, mix.at[2], 7),
        load(data_in, mix.at[3], 8),
        load(rate_in, mix.at[4], 9),
        load(gate_in, gate_v, 10),
        load(down_w_in.at[0], down.at[c], 11),
        load(out_weight_in, out_w, 12),
        load(common_down_in, common_d, 13),
    ]
    loads[0].start()

    barrier = pltpu.get_barrier_semaphore()
    peers = [partner] + [z_dev(d) for d in range(1, n_z)] + [tp_dev(d) for d in range(1, n_tp)]
    for dev in peers:
        pl.semaphore_signal(barrier, inc=1, device_id=dev, device_id_type=MESH)
    for copy in loads[1:5]:
        copy.start()

    r_i = lax.broadcasted_iota(jnp.int32, (group, group), 0)
    c_i = lax.broadcasted_iota(jnp.int32, (group, group), 1)
    mask_v[...] = jnp.where((r_i >> 6) == (c_i >> 6), 1.0, 0.0).astype(BF)
    meta[z] = jnp.concatenate([ids_in[...].astype(F32), factor_in[...]], axis=0)
    loads[0].wait()
    wide = second[...].astype(F32)
    scale = lax.rsqrt(jnp.mean(wide * wide, axis=-1, keepdims=True) + NORM_FLOOR)
    for k in range(n_tp):
        lanes = pl.ds(k * piece, piece)
        rows[k, z] = (
            second[:, lanes].astype(F32) * scale * norm_in[:, lanes]
        ).astype(BF)
    for copy in loads[5:]:
        copy.start()

    pl.semaphore_wait(barrier, len(peers))

    def rows_z(d):
        return send(rows.at[t, z], rows.at[t, z], zs.at[d], zr.at[d], z_dev(d))

    def rows_z_wait(d):
        w = z_at(d)
        return send(rows.at[t, w], rows.at[t, w], zs.at[d], zr.at[d], z_dev(d))

    def meta_z(d):
        return send(meta.at[z], meta.at[z], ms.at[d], mr.at[d], z_dev(d))

    def meta_z_wait(d):
        w = z_at(d)
        return send(meta.at[w], meta.at[w], ms.at[d], mr.at[d], z_dev(d))

    for d in range(1, n_z):
        rows_z(d).start()
    for d in range(1, n_z):
        meta_z(d).start()
    for copy in loads[3:5]:
        copy.wait()
    swap_up = send(gate_up.at[c], gate_up.at[c], ws.at[0], wr.at[0], partner)
    swap_up_in = send(gate_up.at[1 - c], gate_up.at[1 - c], ws.at[0], wr.at[0], partner)
    swap_down = send(down.at[c], down.at[c], ws.at[1], wr.at[1], partner)
    swap_down_in = send(down.at[1 - c], down.at[1 - c], ws.at[1], wr.at[1], partner)
    swap_up.start()

    square = n_tp == 4
    if square:
        x_t, y_t, far_t = t + 1 - 2 * (t % 2), (t + 2) % 4, 3 - t
        x_dev, y_dev = (e, x_t), (e, y_t)

    class Exchange:
        def __init__(self, whole, half, sem_s, sem_r, straight):
            self.whole, self.half, self.sem_s, self.sem_r = whole, half, sem_s, sem_r
            self.relayed = square and not straight

        def copy(self, ref, k, dev):
            return send(ref, ref, self.sem_s(k), self.sem_r(k), dev)

        def first(self):
            if square:
                near = [self.copy(self.whole(t), 1, x_dev), self.copy(self.whole(t), 2, y_dev)]
                far = [self.copy(self.whole(t), 3, (e, far_t))]
                return near + ([] if self.relayed else far)
            return [self.copy(self.whole(t), k, tp_dev(k)) for k in range(1, n_tp)]

        def second(self):
            if self.relayed:
                return [
                    self.copy(self.half(x_t, 0), 3, y_dev),
                    self.copy(self.half(y_t, 1), 0, x_dev),
                ]
            return []

        def start(self):
            for copy in self.first():
                copy.start()

        def near_in(self):
            return [self.copy(self.whole(x_t), 1, x_dev), self.copy(self.whole(y_t), 2, y_dev)]

        def forward(self):
            if self.relayed:
                for came, copy in zip(self.near_in(), self.second()):
                    came.wait_recv()
                    copy.start()

        def finish(self):
            if self.relayed:
                self.copy(self.half(far_t, 0), 3, y_dev).wait_recv()
                self.copy(self.half(far_t, 1), 0, x_dev).wait_recv()
            elif square:
                for came in self.near_in() + [self.copy(self.whole(far_t), 3, (e, far_t))]:
                    came.wait_recv()
            else:
                for k in range(1, n_tp):
                    src = (t - k + n_tp) % n_tp
                    self.copy(self.whole(src), k, tp_dev(k)).wait_recv()

        def sent(self):
            for copy in self.first() + self.second():
                copy.wait_send()

    def straight(kind, d):
        return line and (kind, d) in STRAIGHT

    half_rows = row_count // 2
    shared_x = Exchange(
        lambda src: shared.at[src],
        lambda src, i: shared.at[src, pl.ds(i * half_rows, half_rows)],
        lambda k: cs.at[k], lambda k: cr.at[k], False,
    )

    def rows_x(d):
        zz = z_at(d)
        return Exchange(
            lambda src: rows.at[src, zz],
            lambda src, i: rows.at[src, zz, pl.ds(i * half_rows, half_rows)],
            lambda k: rs.at[d, k], lambda k: rr.at[d, k], straight("rows", d),
        )

    def hidden_x(d):
        zz = z_at(d)
        return Exchange(
            lambda src: hidden.at[src, zz],
            lambda src, i: hidden.at[src, zz, pl.ds(i * cap, cap)],
            lambda k: hs.at[d, k], lambda k: hr.at[d, k], straight("hidden", d),
        )

    def each(low, high, step):
        if high - low <= 4:
            for d in range(low, high):
                step(d)
        else:
            def body(d, carry):
                step(d)
                return carry

            lax.fori_loop(low, high, body, 0)

    def both_dots(zz, weights):
        totals = [None] * len(weights)
        for i, weight in enumerate(weights):
            for k in range(n_tp):
                term = dot(rows[k, zz], weight[:, k * piece : (k + 1) * piece], "nt")
                totals[i] = term if totals[i] is None else totals[i] + term
        return [(silu(total[:, :hid]) * total[:, hid:]).astype(BF) for total in totals]

    for copy in loads[1:3]:
        copy.wait()
    shared[t] = both_dots(z, [common])[0]
    shared_x.start()

    def routes(zz):
        cols = jnp.transpose(meta[zz])
        base = (z * 2).astype(F32)
        return cols, base

    def routed(d):
        zz = z_at(d)
        cols, base = routes(zz)
        lane = lax.broadcasted_iota(jnp.int32, (row_count, 128), 1).astype(F32) + base
        named = jnp.zeros((row_count, 128), F32)
        for k in range(top):
            named = named + jnp.where(cols[:, k : k + 1] == lane, 1.0, 0.0)
        row = lax.broadcasted_iota(jnp.int32, (row_count, row_count), 0)
        col = lax.broadcasted_iota(jnp.int32, (row_count, row_count), 1)
        rank = dot(jnp.where(row > col, 1.0, 0.0).astype(BF), named.astype(BF))
        slot = lax.broadcasted_iota(jnp.int32, (row_count, cap), 1).astype(F32)
        units = both_dots(zz, [gate_up[0], gate_up[1]])
        chosen = [
            jnp.where(
                slot == rank[:, x : x + 1],
                jnp.broadcast_to(named[:, x : x + 1], (row_count, cap)),
                0.0,
            ).astype(BF)
            for x in range(2)
        ]
        packed = [dot(chosen[x], units[x], "tn").astype(BF) for x in range(2)]
        for x in range(2):
            picks[zz, x] = chosen[x]
            hidden[t, zz, pl.ds(x * cap, cap)] = packed[x]
        hidden_x(d).start()

    def relay(d):
        rows_z_wait(d).wait_recv()
        rows_x(d).start()

    stride = SPANS_AT_ONCE if spans % SPANS_AT_ONCE == 0 else 1

    def span_step(i):
        where = [
            (i * stride + j, pl.ds((i * stride + j) * SPAN, SPAN), pl.ds(g * group, group))
            for j in range(stride)
            for g in range(groups)
        ]
        found = local_spans(
            [
                tuple(mix[k, span, lanes] for k in range(5)) + (offset_in[:, lanes],)
                for _, span, lanes in where
            ],
            mask_v[:lane_tile, :lane_tile],
            mask_v[...],
        )
        for (b, span, lanes), (read_state, read_value, move, add) in zip(where, found):
            reads[0, span, lanes] = read_state
            reads[1, span, lanes] = read_value
            steps[0, b, :, lanes] = move
            steps[1, b, :, lanes] = add

    tiles = [pl.ds(g * group, group) for g in range(groups)]
    wide = width // 2

    def small_mask():
        return mask_v[: min(128, wide), : min(128, wide)]

    def compose_own():
        mask = mask_v[:lane_tile, :lane_tile]
        now = [steps[k, 0, :, lanes] for k in range(2) for lanes in tiles]
        for b in range(1, spans):
            now = per_heads([steps[0, b, :, lanes] for lanes in tiles] * 2, now, mask, fine=True)
            for g, lanes in enumerate(tiles):
                now[groups + g] = now[groups + g] + steps[1, b, :, lanes]
        for k in range(2):
            both = now[k * groups : (k + 1) * groups]
            both = both[0] if groups == 1 else jnp.concatenate(both, axis=1)
            for h in range(2):
                pair[c, h, :, k * wide : (k + 1) * wide] = both[
                    :, h * wide : (h + 1) * wide
                ].astype(BF)

    def pair_on(core):
        return send(pair.at[core], pair.at[core], ps.at[0], pr.at[0], partner)

    def chip_z(d, zz):
        return send(chip.at[zz, c], chip.at[zz, c], ps.at[d], pr.at[d], z_dev(d))

    def chip_on(d, half):
        zz = z_at(d)
        return send(chip.at[zz, half], chip.at[zz, half], fs.at[d], fr.at[d], partner)

    def apply(before, now, mask):
        new = per_heads([now[:, :wide].astype(F32)] * len(before), before, mask, fine=True)
        new[-1] = new[-1] + now[:, wide:].astype(F32)
        return new

    def compose_chip():
        pair_on(1 - c).wait_recv()
        first = pair[0, c].astype(F32)
        new = apply([first[:, :wide], first[:, wide:]], pair[1, c], small_mask())
        for k in range(2):
            chip[z, c, :, k * wide : (k + 1) * wide] = new[k].astype(BF)
        for d in range(1, n_z):
            chip_z(d, z).start()

    def chips_forward():
        for d in range(1, n_z):
            chip_z(d, z_at(d)).wait_recv()
            chip_on(d, c).start()

    def finish_mixer():
        for d in range(1, n_z):
            chip_on(d, 1 - c).wait_recv()

        def prefix(i, state):
            return [apply([state[h]], chip[i, h], small_mask())[0] for h in range(2)]

        state = lax.fori_loop(0, z, prefix, [jnp.zeros((HEAD, wide), F32) for _ in range(2)])
        behind = [apply([state[h]], pair[0, h], small_mask())[0] for h in range(2)]
        state = [jnp.where(c == 1, behind[h], state[h]) for h in range(2)]
        if wide != group:
            state = jnp.concatenate(state, axis=1)
            state = [state[:, g * group : (g + 1) * group] for g in range(groups)]
        loads[10].wait()

        def finish_step(b, state):
            span = pl.ds(b * SPAN, SPAN)
            mask, ones = mask_v[:lane_tile, :lane_tile], mask_v[...]
            many = range(groups)
            recepts = [mix[0, span, lanes].astype(F32) for lanes in tiles]
            keys = [mix[1, span, lanes].astype(F32) for lanes in tiles]
            own = [recepts[g] * keys[g] * self_in[:, tiles[g]] for g in many]
            both = per_heads(
                [
                    jnp.concatenate([reads[0, span, lanes], steps[0, b, :, lanes]], axis=0)
                    for lanes in tiles
                ],
                state, mask, fine=True,
            )
            following = [both[g][SPAN:] + steps[1, b, :, tiles[g]] for g in many]
            read = [reads[1, span, tiles[g]] + both[g][:SPAN] for g in many]
            sums = head_sums([jnp.concatenate([read[g], own[g]], axis=0) for g in many], ones)
            apart = [read[g] - sums[g][:SPAN] * (1.0 / HEAD) for g in many]
            squares = head_sums([x * x for x in apart], ones)
            for g, lanes in enumerate(tiles):
                normed = (
                    apart[g]
                    * lax.rsqrt(squares[g] * (1.0 / HEAD) + NORM_FLOOR)
                    * gain_in[:, lanes]
                )
                out = (normed + sums[g][SPAN:] * mix[2, span, lanes].astype(F32)) * gate_v[
                    span, lanes
                ].astype(F32)
                mixed[span, lanes] = out.astype(BF)
            return following

        for b in range(spans):
            state = finish_step(b, state)

    share = positions // n_tp
    wide_cols = min(512, model)

    def project():
        loads[12].wait()
        for i in range(model // wide_cols):
            lanes = pl.ds(i * wide_cols, wide_cols)
            got = dot(mixed[...], out_w[:, lanes]).astype(BF)
            for k in range(n_tp):
                part[k, :, lanes] = got[k * share : (k + 1) * share]

    def part_to(d):
        return send(
            part.at[(t + d) % n_tp], part_in.at[d], os.at[d], orr.at[d], tp_dev(d)
        )

    half_model = model // 2

    def cut(h):
        return pl.ds(h * half_model, half_model)

    def pair_to(h, j):
        k = (x_t + 2 * j) % 4 if h == 0 else (y_t + j * (1 - 2 * (t % 2))) % 4
        dev = x_dev if h == 0 else y_dev
        i = 2 * h + j
        return send(part.at[k, :, cut(h)], part_in.at[j, :, cut(h)], os.at[i], orr.at[i], dev)

    def sum_to(h):
        dev = y_dev if h == 0 else x_dev
        return send(
            part_in.at[2, :, cut(h)], part_in.at[3, :, cut(h)], os.at[4 + h], orr.at[4 + h], dev
        )

    def parts_start():
        if square:
            for h in range(2):
                for j in (1, 0):
                    pair_to(h, j).start()
        else:
            for d in range(1, n_tp):
                part_to(d).start()

    def parts_turn():
        for h in range(2):
            k = y_t if h == 0 else x_t
            pair_to(h, 1).wait_recv()
            part_in[2, :, cut(h)] = (
                part[k, :, cut(h)].astype(F32) + part_in[1, :, cut(h)].astype(F32)
            ).astype(BF)
            sum_to(h).start()

    def parts_sum():
        if square:
            out = []
            for h in range(2):
                pair_to(h, 0).wait_recv()
                sum_to(h).wait_recv()
                out.append(
                    part[t, :, cut(h)].astype(F32)
                    + part_in[0, :, cut(h)].astype(F32)
                    + part_in[3, :, cut(h)].astype(F32)
                )
            return jnp.concatenate(out, axis=1)
        summed = part[t].astype(F32)
        for d in range(1, n_tp):
            part_to(d).wait_recv()
            summed = summed + part_in[d].astype(F32)
        return summed

    def back_to(d):
        return send(back.at[z_at(d)], back_in.at[d], bs.at[d], br.at[d], back_dev(d))

    def routed_out(d):
        zz = z_at(d)
        cols, base = routes(zz)
        hidden_x(d).finish()
        copies = [None, None]
        for x in range(2):
            for k in range(n_tp):
                term = dot(
                    hidden[k, zz, pl.ds(x * cap, cap)], down[x, pl.ds(k * hid, hid)]
                )
                copies[x] = term if copies[x] is None else copies[x] + term
        terms = [dot(picks[zz, x], copies[x].astype(BF)) for x in range(2)]
        total = None
        for x in range(2):
            factor = jnp.zeros((row_count, 1), F32)
            for k in range(top):
                factor = factor + jnp.where(
                    cols[:, k : k + 1] == base + float(x), cols[:, top + k : top + k + 1], 0.0
                )
            term = terms[x] * factor
            total = term if total is None else total + term
        return total

    def send_back(d):
        back[z_at(d)] = routed_out(d).astype(BF)
        back_to(d).start()

    def other(d):
        meta_z_wait(d).wait_recv()
        rows_x(d).finish()
        routed(d)

    for copy in loads[5:10]:
        copy.wait()
    swap_up_in.wait_recv()
    routed(0)
    if line:
        relay(1)
    span_step(0)
    shared_x.forward()
    loads[11].wait()
    swap_down.start()
    for i in range(1, spans // stride):
        span_step(i)
    if line:
        rows_x(1).forward()
    compose_own()
    pair_on(c).start()
    if line:
        relay(2)
    hidden_x(0).forward()
    if line:
        compose_chip()
        other(1)
        rows_x(2).forward()
        relay(3)
        other(2)
        hidden_x(1).forward()
        chips_forward()
        rows_x(3).forward()
        hidden_x(2).forward()
        other(3)
        hidden_x(3).forward()
        swap_down_in.wait_recv()
        send_back(1)
        send_back(2)
        finish_mixer()
        project()
        parts_start()
        send_back(3)
        if square:
            parts_turn()
    else:
        compose_chip()
        each(1, n_z, relay)
        each(1, n_z, lambda d: rows_x(d).forward())
        each(1, n_z, other)
        each(1, n_z, lambda d: hidden_x(d).forward())
        swap_down_in.wait_recv()
        each(1, n_z, send_back)
        chips_forward()
        finish_mixer()
        project()
        parts_start()
    result = routed_out(0)
    loads[13].wait()
    shared_x.finish()
    for k in range(n_tp):
        result = result + dot(shared[k], common_d[pl.ds(k * hid, hid)])

    if square and not line:
        parts_turn()
    summed = parts_sum()
    token_out[...] = summed.astype(BF)

    for d in range(1, n_z):
        back_to(d).wait_recv()
    for d in range(1, n_z):
        result = result + back_in[d].astype(F32)
    expert_out[...] = result.astype(BF)

    swap_up.wait_send()
    swap_down.wait_send()
    for d in range(1, n_z):
        rows_z(d).wait_send()
        meta_z(d).wait_send()
        chip_z(d, z).wait_send()
        chip_on(d, c).wait_send()
        back_to(d).wait_send()
        rows_x(d).sent()
    pair_on(c).wait_send()
    for d in range(n_z):
        hidden_x(d).sent()
    shared_x.sent()
    if square:
        for h in range(2):
            sum_to(h).wait_send()
            for j in range(2):
                pair_to(h, j).wait_send()
    else:
        for k in range(1, n_tp):
            part_to(k).wait_send()


def on_device(n_ep, n_tp, *args):
    (
        receptance, key_tensor, value_tensor, decay_data_input, correction_rate_input,
        mixer_output_gate, decay_channel_offset, head_norm_gain, self_key_weight,
        mixer_output_weight, second_batch_rows, routed_expert_index, routing_output_weight,
        expert_norm_gain, expert_gate_weight, expert_up_weight, expert_down_weight,
        common_expert_gate, common_expert_up, common_expert_down,
    ) = args
    n_z = n_ep // 2
    positions, width = receptance.shape
    row_count, model = second_batch_rows.shape
    top = routed_expert_index.shape[1]
    cap = 3 * row_count * top // (2 * n_ep)
    cap = -(-cap // 16) * 16
    hid = common_expert_gate.shape[0]
    units = common_expert_down.shape[0]
    piece = model // n_tp
    group = min(256, width)
    spans = positions // SPAN
    any_spec = pl.BlockSpec(memory_space=pl.ANY)
    vmem = pl.BlockSpec(memory_space=pltpu.VMEM)
    dma = pltpu.SemaphoreType.DMA
    share = positions // n_tp
    found = pl.pallas_call(
        functools.partial(whole_kernel, (n_z, n_tp, top, cap)),
        out_shape=(
            jax.ShapeDtypeStruct((share, model), BF),
            jax.ShapeDtypeStruct((row_count, piece), BF),
        ),
        in_specs=[any_spec] * 6 + [vmem] * 3 + [any_spec] + [any_spec, vmem, vmem, vmem] + [any_spec] * 6,
        out_specs=(vmem, vmem),
        scratch_shapes=[
            pltpu.VMEM((5, positions, width), BF),
            pltpu.VMEM((positions, width), BF),
            pltpu.VMEM((width, model), BF),
            pltpu.VMEM((row_count, model), BF),
            pltpu.VMEM((n_tp, n_z, row_count, piece), BF),
            pltpu.VMEM((n_z, 2 * top, row_count), F32),
            pltpu.VMEM((2, 2 * hid, model), BF),
            pltpu.VMEM((2, units, piece), BF),
            pltpu.VMEM((2 * hid, model), BF),
            pltpu.VMEM((units, piece), BF),
            pltpu.VMEM((n_z, 2, row_count, cap), BF),
            pltpu.VMEM((n_tp, n_z, 2 * cap, hid), BF),
            pltpu.VMEM((n_tp, row_count, hid), BF),
            pltpu.VMEM((n_tp, share, model), BF),
            pltpu.VMEM((n_tp, share, model), BF),
            pltpu.VMEM((n_z, row_count, piece), BF),
            pltpu.VMEM((n_z, row_count, piece), BF),
            pltpu.VMEM((2, 2, HEAD, width), BF),
            pltpu.VMEM((n_z, 2, HEAD, width), BF),
            pltpu.VMEM((2, positions, width), F32),
            pltpu.VMEM((2, spans, HEAD, width), F32),
            pltpu.VMEM((positions, width), BF),
            pltpu.VMEM((group, group), BF),
            dma((14,)),
            dma((n_z,)), dma((n_z,)), dma((n_z,)), dma((n_z,)),
            dma((n_z, n_tp)), dma((n_z, n_tp)), dma((n_z, n_tp)), dma((n_z, n_tp)),
            dma((n_tp,)), dma((n_tp,)),
            dma((n_z,)), dma((n_z,)), dma((n_z,)), dma((n_z,)),
            dma((max(6, n_tp),)), dma((max(6, n_tp),)),
            dma((n_z,)), dma((n_z,)),
            dma((2,)), dma((2,)),
        ],
        compiler_params=pltpu.CompilerParams(
            collective_id=0, has_side_effects=True, vmem_limit_bytes=60 * 1024 * 1024
        ),
        name="mixer_and_experts",
    )(
        receptance, key_tensor, value_tensor, decay_data_input, correction_rate_input,
        mixer_output_gate, decay_channel_offset[None], head_norm_gain[None],
        self_key_weight[None], mixer_output_weight, second_batch_rows,
        routed_expert_index.T, routing_output_weight.T,
        expert_norm_gain[None], expert_gate_weight, expert_up_weight, expert_down_weight,
        common_expert_gate, common_expert_up, common_expert_down,
    )
    return pl.pallas_call(
        put_kernel,
        out_shape=tuple(jax.ShapeDtypeStruct(x.shape, x.dtype) for x in found),
        in_specs=[vmem] * 2,
        out_specs=(any_spec, any_spec),
        scratch_shapes=[dma((2,))],
        name="put_results",
    )(*found)


def put_kernel(token_in, expert_in, token_out, expert_out, sems):
    copies = [
        pltpu.make_async_copy(token_in, token_out, sems.at[0]),
        pltpu.make_async_copy(expert_in, expert_out, sems.at[1]),
    ]
    for copy in copies:
        copy.start()
    for copy in copies:
        copy.wait()


def solution(mesh):
    in_specs = (
        (P("ep", "tp"),) * 6
        + (P("tp"),) * 3
        + (P("tp", None),)
        + (P("ep", None),) * 3
        + (P(), P("ep", "tp", None), P("ep", "tp", None), P("ep", None, "tp"))
        + (P("tp", None), P("tp", None), P(None, "tp"))
    )
    out_specs = (P(("ep", "tp"), None), P("ep", "tp"))
    return jax.shard_map(
        functools.partial(on_device, mesh.shape["ep"], mesh.shape["tp"]),
        mesh=mesh, in_specs=in_specs, out_specs=out_specs, check_vma=False,
    )
```
